512 devices in a mesh: ep: 32 (over z, x), tp: 16 (over y, core).
Axes of the slice: x: 4, y: 8, z: 8, core: 2. Of those that a mesh axis runs over, the one named last changes fastest.
Arguments:
- x_path: bfloat16 [32768, 2048], P('ep', 'tp'), may hold values from -6 to 6
- gate_path: bfloat16 [32768, 2048], P('ep', 'tp'), may hold values from -6 to 6
- conv_taps: float32 [4, 2048], P(None, 'tp'), may hold values from -3 to 3
- decay_gate_w: bfloat16 [2, 16, 128, 128], P(None, 'tp'), may hold values from -0.5 to 0.5
- input_gate_w: bfloat16 [2, 16, 128, 128], P(None, 'tp'), may hold values from -0.5 to 0.5
- decay_rate: float32 [2, 2048], P(None, 'tp'), may hold values from 0 to 1, as said below
- decay_shift: float32 [32768, 16], P('ep', 'tp'), may hold values from -1 to 0, as said below
- expert_in: bfloat16 [8192, 2048], P('ep'), may hold values from -6 to 6
- norm_gain: float32 [2048], replicated, may hold values from 0.1 to 1.9
- routes: int32 [8192, 2], P('ep'), may hold values from 0 to 31, all different within a row; in each aligned block of 16 rows (0 to 15, 16 to 31, ...) at most 2 rows name the same one
- route_scores: float32 [8192, 2], P('ep'), may hold values from 0.1 to 1
- gate_weight: bfloat16 [32, 2048, 4096], P('ep', None, 'tp'), may hold values from -0.125 to 0.125
- up_weight: bfloat16 [32, 2048, 4096], P('ep', None, 'tp'), may hold values from -0.125 to 0.125
- down_weight: bfloat16 [32, 4096, 2048], P('ep', 'tp'), may hold values from -0.09375 to 0.09375
Outputs:
- recurrent_out: bfloat16 [32768, 2048], P('ep', 'tp')
- expert_out: bfloat16 [8192, 2048], P(('ep', 'tp'))
The draws below stay inside these ranges and needn't reach their ends.
Inputs may be any that keep to these rules, and one draw needn't show every extreme that they name: `routes`: in each aligned block of 16 rows no expert is named by more than 2 rows, and in some block some expert is named by exactly 2 rows; each row names 2 different experts. `decay_rate`: positive rates. `decay_shift`: never positive.
All inputs are finite; a program needn't handle non-finite values.
Results may differ from the reference program's by a relative error of at most 0.019.
Values may be sent and summed in bfloat16 or wider, within the bound.
A program may use at most 64 MiB of HBM per device.

```python
import math
import jax
import jax.numpy as jnp
import numpy as np
from jax import lax

D = 2048
RECURRENT_HEADS = 16
HEAD_DIM = 128
WIDTH = 2048
FF = 4096
FF_DEV = 256
TOP_K = 2
EXPERTS = 32
MIX_ROWS = 1024
MIXER_TOKENS = 32768
EXP_ROWS = 16
EXP_TOKENS = 8192
CAPACITY = 2
N_TP = 16


def draw_decay_rate(key, part):
    pick_key, fast_key, slow_key = jax.random.split(key, 3)
    fast_share = 0.5
    is_fast = jax.random.uniform(pick_key, (2, RECURRENT_HEADS, 1), jnp.float32) < fast_share
    forget_span = float(min(40, MIX_ROWS // 2))
    fast_rate = jnp.exp(jax.random.uniform(fast_key, (2, RECURRENT_HEADS, HEAD_DIM), jnp.float32, math.log(0.5), math.log(1.5))) / (4.0 * forget_span)
    slow_rate = jnp.exp(jax.random.uniform(slow_key, (2, RECURRENT_HEADS, HEAD_DIM), jnp.float32, math.log(0.5), math.log(2.0))) * (0.12 / MIXER_TOKENS)
    return jnp.where(is_fast, fast_rate, slow_rate).reshape(2, RECURRENT_HEADS * HEAD_DIM)


def draw_decay_shift(key, part):
    block_key, location_random_key, depth_random_key = jax.random.split(key, 3)
    block_count = MIXER_TOKENS // MIX_ROWS
    per_block = -jax.random.uniform(block_key, (block_count, 1, RECURRENT_HEADS), jnp.float32, 0.2, 2.0) * (0.3 / MIXER_TOKENS)
    baseline_level = jnp.broadcast_to(per_block, (block_count, MIX_ROWS, RECURRENT_HEADS)).reshape(MIXER_TOKENS, RECURRENT_HEADS)
    spike_locations = jax.random.randint(location_random_key, (2, RECURRENT_HEADS), 0, MIXER_TOKENS)
    spike_depths = jnp.log(jax.random.uniform(depth_random_key, (2, RECURRENT_HEADS), jnp.float32, 0.5, 0.8))
    token_positions = jnp.arange(MIXER_TOKENS, dtype=jnp.int32)[:, None]
    initial_spike = jnp.where(token_positions == spike_locations[0][None, :], spike_depths[0][None, :], 0.0)
    following_spike = jnp.where(token_positions == spike_locations[1][None, :], spike_depths[1][None, :], 0.0)
    return baseline_level + initial_spike + following_spike


def steps_of(key, extent, cuts, least, top_value):
    factor_of, own = 1.0, jax.random.fold_in(key, 6)
    for dim, shards_of in cuts:
        draws = jnp.exp(jax.random.uniform(jax.random.fold_in(own, dim), (shards_of,), jnp.float32, least / len(cuts), top_value / len(cuts)))
        factor_of = factor_of * jnp.repeat(draws, extent[dim] // shards_of).reshape([-1 if axis == dim else 1 for axis in range(len(extent))])
    return factor_of


def routed_block(key, own, number, rows, number_of, top, bound, slope):
    sequence = jax.random.permutation(key, number_of)
    crowded, usual = load_shares(number_of, rows * top, bound, slope, True), load_shares(number_of, rows * top, bound, slope, False)
    places = jnp.arange(number_of)

    def named(lengths, offset_by):
        used = int((lengths > 0).sum())
        fixed = max(1, used // 4)
        passed = fixed + (places - fixed + offset_by * (used - fixed)) % max(1, number_of - fixed)
        return jnp.zeros((number_of,), jnp.int32).at[sequence[jnp.where(places < fixed, places, passed)]].set(jnp.asarray(lengths, jnp.int32))

    lengths = jnp.where(number % 4 == 0, named(crowded, number // 4), named(usual, number - number // 4 - 1))
    mixed = jax.random.permutation(jax.random.fold_in(own, 3), number_of)
    giver, taker = mixed[0:number_of // 2 * 2:2], mixed[1:number_of // 2 * 2:2]
    slack = jnp.minimum(lengths[giver] - 1, bound - lengths[taker]) // 2
    slack = jnp.where((giver == sequence[0]) | (taker == sequence[0]) | (lengths[taker] == 0), 0, jnp.maximum(slack, 0))
    passed = jax.random.randint(jax.random.fold_in(own, 4), (number_of // 2,), 0, 1 << 20) % (slack + 1)
    lengths = lengths.at[giver].add(-passed).at[taker].add(passed)
    labels = jnp.searchsorted(jnp.cumsum(lengths), jnp.arange(rows * top), side="right").astype(jnp.int32)
    listing = labels.reshape(top, rows).T
    listing = listing[jax.random.permutation(jax.random.fold_in(own, 1), rows)]
    offset_by = jax.random.randint(jax.random.fold_in(own, 2), (rows, 1), 0, top)
    return jnp.take_along_axis(listing, (jnp.arange(top)[None, :] + offset_by) % top, axis=1)


def load_shares(count, total, bound, lean, full):
    weights = [(1 << 20) // math.isqrt(rank ** lean) + 1 for rank in range(1, count + 1)]
    largest = bound if full else min(bound, max(-(-total // count), total * weights[0] // sum(weights)))
    least = 1 if total - largest >= count - 1 else 0
    holding, surplus = [largest] + [least] * (count - 1), total - largest - least * (count - 1)
    while surplus > 0:
        movable = [i for i in range(1, count) if holding[i] < largest] or [i for i in range(1, count) if holding[i] < bound]
        mass, remaining = sum([weights[i] for i in movable]), surplus
        for i in movable:
            addition = min(bound - holding[i], max(1, remaining * weights[i] // mass), surplus)
            holding[i] = holding[i] + addition
            surplus = surplus - addition
    return np.array(holding)


def noise(own_key, dims, width, reach, shards=(), kind=jnp.bfloat16):
    values = width * jax.random.normal(own_key, dims, jnp.float32)
    if shards:
        values = values * steps_of(own_key, dims, shards, -0.22, 0.18)
    return jnp.clip(values, -reach, reach).astype(kind)


def setup_inputs(seed: int = 0) -> dict:
    splits = jax.random.split(jax.random.key(seed), 15)
    x_path = noise(splits[0], (MIXER_TOKENS, WIDTH), 1.0, 6.0, ((0, 32), (1, 16)))
    gate_path = noise(splits[1], (MIXER_TOKENS, WIDTH), 1.0, 6.0, ((0, 32), (1, 16)))
    conv_taps = noise(splits[2], (4, WIDTH), 0.5, 3.0, ((1, 16),), jnp.float32)
    decay_gate_w = noise(splits[3], (2, RECURRENT_HEADS, HEAD_DIM, HEAD_DIM), HEAD_DIM ** -0.5, 0.5, ((1, 16),))
    input_gate_w = noise(splits[4], (2, RECURRENT_HEADS, HEAD_DIM, HEAD_DIM), HEAD_DIM ** -0.5, 0.5, ((1, 16),))
    decay_rate = draw_decay_rate(jax.random.fold_in(splits[14], 71), 0)
    decay_shift = draw_decay_shift(jax.random.fold_in(splits[14], 71), 0)
    expert_in = noise(splits[7], (EXP_TOKENS, D), 1.0, 6.0, ((0, 32),))
    norm_gain = jnp.clip(1.0 + 0.18 * jax.random.normal(splits[8], (D,), jnp.float32), 0.1, 1.9)
    routes_keys = jax.random.split(jax.random.fold_in(splits[9], 1), EXP_TOKENS // EXP_ROWS)
    routes_turns = jax.random.permutation(jax.random.fold_in(splits[9], 3), EXP_TOKENS // EXP_ROWS)
    routes = jax.vmap(lambda own, number: routed_block(jax.random.fold_in(splits[9], 2), own, number, EXP_ROWS, EXPERTS, TOP_K, CAPACITY, 1))(routes_keys, routes_turns).reshape((EXP_TOKENS, TOP_K))
    route_scores = jnp.clip(jnp.exp(math.log(1.0) - 2.3025851 * jax.random.uniform(splits[10], (EXP_TOKENS, TOP_K), jnp.float32) ** steps_of(splits[10], (EXP_TOKENS, TOP_K), ((0, 32),), -0.2, 0.2)), 0.1, 1.0)
    gate_weight = noise(splits[11], (EXPERTS, D, FF), D ** -0.5, 0.125, ((0, 32), (2, 16)))
    up_weight = noise(splits[12], (EXPERTS, D, FF), D ** -0.5, 0.125, ((0, 32), (2, 16)))
    down_weight = noise(splits[13], (EXPERTS, FF, D), FF ** -0.5, 0.09375, ((0, 32), (1, 16)))
    return {"x_path": x_path, "gate_path": gate_path, "conv_taps": conv_taps, "decay_gate_w": decay_gate_w, "input_gate_w": input_gate_w, "decay_rate": decay_rate, "decay_shift": decay_shift, "expert_in": expert_in, "norm_gain": norm_gain, "routes": routes, "route_scores": route_scores, "gate_weight": gate_weight, "up_weight": up_weight, "down_weight": down_weight}


EPSILON = 1e-06

def link_pairs(earlier, later):
    return (earlier[0] * later[0], later[0] * earlier[1] + later[1])

def block_gates(conv_block, weights):
    length = conv_block.shape[0]
    grouped = conv_block.astype(jnp.float32).reshape(length, RECURRENT_HEADS, HEAD_DIM)
    preact = jnp.einsum('thi,hij->thj', grouped, weights.astype(jnp.float32))
    return jax.nn.sigmoid(preact).reshape(length, WIDTH)

def chain_states(conv_out, decay_weights, input_weights, rate, shift):
    length = conv_out.shape[0]
    span_rows = math.gcd(length, 512)
    span_count = length // span_rows

    def advance(carry, inputs):
        conv_block, shift_block = inputs
        decay_gate = block_gates(conv_block, decay_weights)
        input_gate = block_gates(conv_block, input_weights)
        log_decay = -8.0 * decay_gate * rate + jnp.repeat(shift_block, HEAD_DIM, axis=1)
        drive = jnp.sqrt(-jnp.expm1(2.0 * log_decay)) * input_gate * conv_block.astype(jnp.float32)
        decay = jnp.exp(log_decay)
        drive = drive.at[0].add(decay[0] * carry)
        states = lax.associative_scan(link_pairs, (decay, drive), axis=0)[1]
        return (states[-1], states)
    initial = jnp.zeros((WIDTH,), jnp.float32)
    blocks_in = (conv_out.reshape(span_count, span_rows, WIDTH), shift.reshape(span_count, span_rows, RECURRENT_HEADS))
    _, states = lax.scan(advance, initial, blocks_in)
    return states.reshape(length, WIDTH)

def recurrence_half(x_path, gate_path, conv_taps, decay_gate_w, input_gate_w, decay_rate, decay_shift):
    length = x_path.shape[0]
    padded = jnp.pad(x_path.astype(jnp.float32), ((2, 1), (0, 0)))
    conv_sum = jnp.zeros((length, WIDTH), jnp.float32)
    for offset in range(4):
        conv_sum = conv_sum + padded[offset:offset + length] * conv_taps[offset]
    conv_out = conv_sum.astype(jnp.bfloat16)
    forward_state = chain_states(conv_out, decay_gate_w[0], input_gate_w[0], decay_rate[0], decay_shift)
    backward_state = chain_states(conv_out[::-1], decay_gate_w[1], input_gate_w[1], decay_rate[1], decay_shift[::-1])[::-1]
    gated = jax.nn.gelu(gate_path.astype(jnp.float32))
    return ((forward_state + backward_state) * gated).astype(jnp.bfloat16)

def slot_ranks(routes):
    tokens = routes.shape[0]
    block_count = tokens // EXP_ROWS
    flattened = routes.reshape(block_count, EXP_ROWS * TOP_K)
    onehot = (flattened[:, :, None] == jnp.arange(EXPERTS, dtype=jnp.int32)[None, None, :]).astype(jnp.int32)
    earlier = lax.optimization_barrier(jnp.sum((jnp.cumsum(onehot, axis=1) - onehot) * onehot, axis=2))
    return earlier.reshape(tokens, TOP_K).astype(jnp.int32)

def expert_half(expert_in, norm_gain, routes, route_scores, gate_weight, up_weight, down_weight):
    tokens = expert_in.shape[0]
    block_count = tokens // EXP_ROWS
    wide_in = expert_in.astype(jnp.float32)
    scale = lax.rsqrt(lax.optimization_barrier(jnp.mean(wide_in * wide_in, axis=1, keepdims=True)) + EPSILON)
    normed = (wide_in * scale * norm_gain).astype(jnp.bfloat16)
    ranks = slot_ranks(routes)
    block_of = (jnp.arange(tokens, dtype=jnp.int32) // EXP_ROWS)[:, None]
    columns = (block_of * CAPACITY + ranks).astype(jnp.int32)
    token_ids = jnp.broadcast_to(jnp.arange(tokens, dtype=jnp.int32)[:, None], routes.shape)
    table = jnp.full((EXPERTS, block_count * CAPACITY), tokens, jnp.int32)
    table = table.at[routes, columns].set(token_ids)
    padded = jnp.concatenate([normed, jnp.zeros((1, D), jnp.bfloat16)], axis=0)

    def one_expert(inputs):
        row_index, gate_mat, up_mat, down_mat = inputs
        picked_rows = padded[row_index]
        gate_pre = jnp.dot(picked_rows, gate_mat, preferred_element_type=jnp.float32)
        up_pre = jnp.dot(picked_rows, up_mat, preferred_element_type=jnp.float32)
        hidden = (jax.nn.silu(gate_pre) * up_pre).astype(jnp.bfloat16)
        grouped = hidden.reshape(-1, N_TP, FF_DEV).astype(jnp.float32)
        down_groups = down_mat.reshape(N_TP, FF_DEV, D).astype(jnp.float32)
        partial_value = jnp.einsum('ngf,gfd->gnd', grouped, down_groups)
        rounded = lax.optimization_barrier(partial_value.astype(jnp.bfloat16)).astype(jnp.float32)
        return lax.optimization_barrier(jnp.sum(rounded, axis=0)).astype(jnp.bfloat16)
    outputs = lax.map(one_expert, (table, gate_weight, up_weight, down_weight))
    chosen = outputs[routes, columns]
    shares = route_scores / lax.optimization_barrier(jnp.sum(route_scores, axis=1, keepdims=True))
    return lax.optimization_barrier(jnp.sum(chosen.astype(jnp.float32) * shares[:, :, None], axis=1)).astype(jnp.bfloat16)

def reference(x_path, gate_path, conv_taps, decay_gate_w, input_gate_w, decay_rate, decay_shift, expert_in, norm_gain, routes, route_scores, gate_weight, up_weight, down_weight):
    recurrent_out = recurrence_half(x_path, gate_path, conv_taps, decay_gate_w, input_gate_w, decay_rate, decay_shift)
    expert_out = expert_half(expert_in, norm_gain, routes, route_scores, gate_weight, up_weight, down_weight)
    return (recurrent_out, expert_out)
```

```python
import functools

import jax
import jax.numpy as jnp
from jax import lax
from jax.experimental import pallas as pl
from jax.experimental.pallas import tpu as pltpu
from jax.sharding import PartitionSpec as P

BF = jnp.bfloat16
F32 = jnp.float32
I32 = jnp.int32
MESH = pl.DeviceIdType.MESH
EPSILON = 1e-06
LANES = 128
EXIT = 16


def log2(n):
    return n.bit_length() - 1


def iota(shape, dim):
    return lax.broadcasted_iota(I32, shape, dim)


def shr(x, n):
    return lax.shift_right_logical(x, jnp.full(x.shape, n, I32))


def dot(a, b):
    return jnp.dot(a, b, preferred_element_type=F32)


def one_hot(mask):
    return jnp.where(mask, 1.0, 0.0).astype(BF)


def one_minus_square(log_a, a):
    z = 2.0 * log_a
    series = 1.0 + z * (1 / 2 + z * (1 / 6 + z * (1 / 24 + z * (1 / 120 + z * (1 / 720)))))
    return jnp.where(z > -0.25, -z * series, 1.0 - a * a)


def layer(
    E,
    T,
    x_hbm,
    gate_hbm,
    ein_hbm,
    wg_hbm,
    wu_hbm,
    wd_hbm,
    taps,
    dgw,
    igw,
    rate,
    shift,
    gain,
    routes,
    routes_t,
    scores,
    rec_out,
    exp_out,
    xraw,
    gatev,
    ein,
    wg,
    wu,
    wd,
    halo,
    xpad,
    sh,
    cperm,
    af,
    bf,
    ab,
    bb,
    ynat,
    seg,
    carry_send,
    carry_recv,
    dsp,
    xb,
    acc,
    perm,
    hp,
    part,
    sibp,
    rs_send,
    rs_recv,
    stk,
    ret_send,
    ret_recv,
    c_hi,
    c_lo,
    load_sem,
    halo_ss,
    halo_rs,
    carry_ss,
    carry_rs,
    dsp_ss,
    dsp_rs,
    ag_ss,
    ag_rs,
    sib_ss,
    sib_rs,
    sp_ss,
    sp_rs,
    rs_ss,
    rs_rs,
    ret_ss,
    ret_rs,
):
    NY, H = T // 2, T // 4
    S = xraw.shape[0]
    NS = S // 8
    R, D = ein.shape
    F = wg.shape[1]
    HALF = D // 2
    N = E * T
    lT, lE, lNY = log2(T), log2(E), log2(NY)

    e = lax.axis_index("ep")
    t = lax.axis_index("tp")
    y = t // 2
    c = t % 2
    sib_t = y * 2 + (1 - c)
    right_t = ((y + 1) % NY) * 2 + c
    left_t = ((y + NY - 1) % NY) * 2 + c
    ep_next = (e + 1) % E
    ep_prev = (e + E - 1) % E

    loads = [
        pltpu.make_async_copy(src, dst, load_sem.at[i])
        for i, (src, dst) in enumerate(
            ((ein_hbm, ein), (x_hbm, xraw), (wg_hbm, wg), (wu_hbm, wu), (gate_hbm, gatev), (wd_hbm, wd))
        )
    ]
    for load in loads:
        load.start()

    barrier = pltpu.get_barrier_semaphore()

    def greet(i, _):
        pl.semaphore_signal(barrier, inc=1, device_id=((e + i) % E, t), device_id_type=MESH)
        return 0

    lax.fori_loop(1, E, greet, 0)
    for peer in (sib_t, right_t, left_t):
        pl.semaphore_signal(barrier, inc=1, device_id=(e, peer), device_id_type=MESH)

    named_t = one_hot((routes_t[0:1, :] == iota((E, R), 0)) | (routes_t[1:2, :] == iota((E, R), 0)))
    rr, rc = iota((R, R), 0), iota((R, R), 1)
    earlier_t = one_hot((shr(rr, 4) == shr(rc, 4)) & (rr < rc))
    rank_t = dot(named_t, earlier_t)
    loads[0].wait()
    total = jnp.zeros((R, LANES), F32)
    for j in range(D // LANES):
        tile = ein[:, j * LANES : (j + 1) * LANES].astype(F32)
        total = total + tile * tile
    scale = lax.rsqrt(jnp.sum(total, axis=1, keepdims=True) * (1.0 / D) + EPSILON)
    own_columns = pl.ds(pl.multiple_of(t * LANES, LANES), LANES)
    normed = (ein[:, own_columns].astype(F32) * scale * gain[pl.ds(t, 1), :]).astype(BF)
    spread = one_hot(shr(iota((N, E), 0), lT) == iota((N, E), 1))
    in_block = (iota((N, R), 0) & (T - 1)) == shr(iota((N, R), 1), 4)
    for w in range(2):
        chosen = jnp.where(rank_t == float(w), named_t.astype(F32), 0.0).astype(BF)
        selector = jnp.where(in_block, dot(spread, chosen), 0.0).astype(BF)
        dsp[w] = dot(selector, normed).astype(BF)

    loads[1].wait()
    pl.semaphore_wait(barrier, E + 2)

    tail = pltpu.make_async_remote_copy(
        xraw.at[pl.ds(S - EXIT, EXIT)], halo.at[0], halo_ss.at[0], halo_rs.at[0],
        device_id=(ep_next, t), device_id_type=MESH,
    )
    head = pltpu.make_async_remote_copy(
        xraw.at[pl.ds(0, EXIT)], halo.at[1], halo_ss.at[1], halo_rs.at[1],
        device_id=(ep_prev, t), device_id_type=MESH,
    )
    tail.start()
    head.start()

    own_rows = pl.ds(pl.multiple_of(e * T, T), T)
    for w in range(2):

        def send(i, _, w=w):
            peer = (e + i) % E
            pltpu.make_async_remote_copy(
                dsp.at[w, pl.ds(pl.multiple_of(peer * T, T), T)],
                xb.at[w, y, c, own_rows],
                dsp_ss.at[w],
                dsp_rs.at[w],
                device_id=(peer, t),
                device_id_type=MESH,
            ).start()
            return 0

        lax.fori_loop(1, E, send, 0)
        xb[w, y, c, own_rows] = dsp[w, own_rows]

    n0, n1 = iota((N, N), 0), iota((N, N), 1)
    perm_block = (shr(n0, lE) & (NY - 1)) * 2 + shr(n0, lE + lNY)
    perm[...] = one_hot((shr(n1, lT) == (n0 & (E - 1))) & ((n1 & (T - 1)) == perm_block))

    own_block = pl.ds(pl.multiple_of(t * EXIT, EXIT), EXIT)
    block_routes = routes[own_block, :]
    block_scores = scores[own_block, :]
    shares = block_scores / jnp.sum(block_scores, axis=1, keepdims=True)
    ids = iota((EXIT, E), 1)
    first = block_routes[:, 0:1] == ids
    second = block_routes[:, 1:2] == ids
    below = one_hot(iota((EXIT, EXIT), 1) < iota((EXIT, EXIT), 0))
    block_rank = dot(below, one_hot(first | second))
    share_of = jnp.where(first, shares[:, 0:1], 0.0) + jnp.where(second, shares[:, 1:2], 0.0)
    rows_out = one_hot((iota((T * EXIT, EXIT), 0) & (EXIT - 1)) == iota((T * EXIT, EXIT), 1))
    columns_out = one_hot(iota((E, N), 0) == shr(iota((E, N), 1), lT))
    same_tile = shr(iota((T * EXIT, N), 0), 4) == (iota((T * EXIT, N), 1) & (T - 1))
    for w in range(2):
        weight = jnp.where(block_rank == float(w), share_of, 0.0)
        high = weight.astype(BF)
        low = (weight - high.astype(F32)).astype(BF)
        for piece, table in ((high, c_hi), (low, c_lo)):
            wide = dot(dot(rows_out, piece).astype(BF), columns_out)
            table[w] = jnp.where(same_tile, wide, 0.0).astype(BF)

    xpad[pl.ds(EXIT, S), :] = xraw[...].astype(F32)
    for s in range(NS):
        sh[pl.ds(s * 8, 8), :] = jnp.broadcast_to(shift[:, s : s + 1], (8, LANES))
    tail.wait_recv()
    head.wait_recv()
    xpad[pl.ds(0, EXIT), :] = jnp.where(e > 0, halo[0].astype(F32), 0.0)
    xpad[pl.ds(EXIT + S, EXIT), :] = jnp.where(e < E - 1, halo[1].astype(F32), 0.0)

    def strided(s):
        return xpad[pl.ds(EXIT + s, 8, stride=NS), :]

    tap = [taps[k : k + 1, :] for k in range(4)]

    def conv(s, held):
        v0, v1, v2 = held
        v3 = strided(s + 1)
        value = v0 * tap[0] + v1 * tap[1] + v2 * tap[2] + v3 * tap[3]
        cperm[pl.ds(pl.multiple_of(s * 8, 8), 8), :] = value.astype(BF).astype(F32)
        return v1, v2, v3

    lax.fori_loop(0, NS, conv, (strided(-2), strided(-1), strided(0)), unroll=8)

    CH = min(128, S)

    def gates(i, _):
        rows = pl.ds(pl.multiple_of(i * CH, CH), CH)
        value = cperm[rows, :]
        value_b = value.astype(BF)
        shift_here = sh[rows, :]
        for d, (a_ref, b_ref) in enumerate(((af, bf), (ab, bb))):
            decay_gate = jax.nn.sigmoid(dot(value_b, dgw[d, 0]))
            input_gate = jax.nn.sigmoid(dot(value_b, igw[d, 0]))
            log_decay = -8.0 * decay_gate * rate[d : d + 1, :] + shift_here
            decay = jnp.exp(log_decay)
            rest = one_minus_square(log_decay, decay)
            root = rest * lax.rsqrt(jnp.maximum(rest, 1e-37))
            a_ref[rows, :] = decay
            b_ref[rows, :] = root * input_gate * value
        return 0

    lax.fori_loop(0, S // CH, gates, 0)

    def at(s):
        return pl.ds(pl.multiple_of(s * 8, 8), 8)

    def summing(s, held):
        hf, pf, hb, pb = held
        a, b = af[at(s), :], bf[at(s), :]
        a2, b2 = ab[at(NS - 1 - s), :], bb[at(NS - 1 - s), :]
        return a * hf + b, a * pf, a2 * hb + b2, a2 * pb

    zero, one = jnp.zeros((8, LANES), F32), jnp.ones((8, LANES), F32)
    hf, pf, hb, pb = lax.fori_loop(0, NS, summing, (zero, one, zero, one), unroll=8)
    for k, value in enumerate((pf, hf, pb, hb)):
        seg[k] = value

    def segment(k, g):
        return seg[k, g : g + 1, :]

    ones = jnp.ones((1, LANES), F32)
    fa, fb, ba, bb_ = ones, ones * 0.0, ones, ones * 0.0
    for g in range(8):
        fa, fb = segment(0, g) * fa, segment(0, g) * fb + segment(1, g)
        ba, bb_ = segment(2, 7 - g) * ba, segment(2, 7 - g) * bb_ + segment(3, 7 - g)
    summary = jnp.concatenate([fa, fb, ba, bb_, jnp.zeros((4, LANES), F32)], axis=0)
    carry_send[...] = summary
    carry_recv[e] = summary

    def send_carry(i, _):
        pltpu.make_async_remote_copy(
            carry_send, carry_recv.at[e], carry_ss, carry_rs,
            device_id=((e + i) % E, t), device_id_type=MESH,
        ).start()
        return 0

    lax.fori_loop(1, E, send_carry, 0)

    def gather_copy(w, direction, hop, rows):
        source = (y + NY - hop) % NY if direction == 0 else (y + hop) % NY
        block = xb.at[w, source, c, rows]
        return pltpu.make_async_remote_copy(
            block, block, ag_ss.at[w, direction, hop], ag_rs.at[w, direction, hop],
            device_id=(e, right_t if direction == 0 else left_t), device_id_type=MESH,
        )

    def arrived_gather(w, direction, hop, rows):
        source = (y + 2 * NY - hop - 1) % NY if direction == 0 else (y + hop + 1) % NY
        block = xb.at[w, source, c, rows]
        pltpu.make_async_copy(block, block, ag_rs.at[w, direction, hop]).wait()

    whole = pl.ds(0, N)
    halves = (pl.ds(0, N // 2), pl.ds(N // 2, N // 2))

    def forward(w, direction, hop):
        if isinstance(hop, int):
            gather_copy(w, direction, hop, halves[direction] if hop == H - 1 else whole).start()

    def sibling_copy(w, source, index):
        block = xb.at[w, source, c]
        return pltpu.make_async_remote_copy(
            block, block, sib_ss.at[w, index], sib_rs.at[w, index],
            device_id=(e, sib_t), device_id_type=MESH,
        )

    def sibling_arrived(w, source, index):
        block = xb.at[w, source, 1 - c]
        pltpu.make_async_copy(block, block, sib_rs.at[w, index]).wait()

    def multiply(w, source, fresh):
        rows = jnp.concatenate([xb[w, source, 0], xb[w, source, 1]], axis=1)
        depth = pl.ds(pl.multiple_of(source * 2 * LANES, 2 * LANES), 2 * LANES)
        for k, weight in enumerate((wg, wu)):
            product = dot(rows, weight[depth, :])
            if fresh:
                acc[w, k] = product
            else:
                acc[w, k] += product

    arrivals = pl.ds(0, (E - 1) * T)
    for w in range(2):
        block = xb.at[w, y, c, arrivals]
        pltpu.make_async_copy(block, block, dsp_rs.at[w]).wait()
        forward(w, 0, 0)
        forward(w, 1, 0)
        sibling_copy(w, y, 0).start()

    pltpu.make_async_copy(
        carry_recv.at[pl.ds(0, E - 1)], carry_recv.at[pl.ds(0, E - 1)], carry_rs
    ).wait()

    def fold(i, held):
        f, b = held
        one_way = carry_recv[i]
        j = E - 1 - i
        other = carry_recv[j]
        f = jnp.where(i < e, one_way[0:1] * f + one_way[1:2], f)
        b = jnp.where(j > e, other[2:3] * b + other[3:4], b)
        return f, b

    f, b = lax.fori_loop(0, E, fold, (ones * 0.0, ones * 0.0))
    f_rows, b_rows = [f], [b]
    for g in range(7):
        f_rows.append(segment(0, g) * f_rows[-1] + segment(1, g))
        b_rows.insert(0, segment(2, 7 - g) * b_rows[0] + segment(3, 7 - g))
    f_in, b_in = jnp.concatenate(f_rows, axis=0), jnp.concatenate(b_rows, axis=0)

    def states(s, held):
        hf, hb = held
        r = NS - 1 - s
        hf = af[at(s), :] * hf + bf[at(s), :]
        hb = ab[at(r), :] * hb + bb[at(r), :]
        bf[at(s), :] = hf
        bb[at(r), :] = hb
        return hf, hb

    lax.fori_loop(0, NS, states, (f_in, b_in), unroll=8)

    def natural(s, _):
        ynat[pl.ds(s, 8, stride=NS), :] = bf[at(s), :] + bb[at(s), :]
        return 0

    lax.fori_loop(0, NS, natural, 0, unroll=8)
    loads[4].wait()

    def finish(i, _):
        rows = pl.ds(pl.multiple_of(i * CH, CH), CH)
        rec_out[rows, :] = (ynat[rows, :] * jax.nn.gelu(gatev[rows, :].astype(F32))).astype(BF)
        return 0

    lax.fori_loop(0, S // CH, finish, 0)

    loads[2].wait()
    loads[3].wait()
    for w in range(2):
        sibling_arrived(w, y, 0)
        multiply(w, y, True)

    for hop in range(1, H):
        rights, lefts = (y + NY - hop) % NY, (y + hop) % NY
        for w in range(2):
            arrived_gather(w, 0, hop - 1, whole)
            forward(w, 0, hop)
            arrived_gather(w, 1, hop - 1, whole)
            forward(w, 1, hop)
            sibling_copy(w, rights, 2 * hop - 1).start()
            sibling_copy(w, lefts, 2 * hop).start()
        for w in range(2):
            sibling_arrived(w, rights, 2 * hop - 1)
            multiply(w, rights, False)
            sibling_arrived(w, lefts, 2 * hop)
            multiply(w, lefts, False)

    far = (y + H) % NY
    for w in range(2):
        arrived_gather(w, 0, H - 1, halves[0])
        arrived_gather(w, 1, H - 1, halves[1])
        sibling_copy(w, far, NY - 1).start()

    def reduce_copy(w, direction, step):
        return pltpu.make_async_remote_copy(
            rs_send.at[w, direction, step], rs_recv.at[w, direction, step],
            rs_ss.at[w, direction, step], rs_rs.at[w, direction, step],
            device_id=(e, right_t if direction == 0 else left_t), device_id_type=MESH,
        )

    def pair_copy(w, direction):
        return pltpu.make_async_remote_copy(
            part.at[w, direction, 1 - c], sibp.at[w, direction],
            sp_ss.at[w, direction], sp_rs.at[w, direction],
            device_id=(e, sib_t), device_id_type=MESH,
        )

    def pair_sum(w, direction, to):
        return part[w, direction, c, to].astype(F32) + sibp[w, direction, to].astype(F32)

    loads[5].wait()
    TILE = min(256, HALF)
    for w in range(2):
        sibling_arrived(w, far, NY - 1)
        multiply(w, far, False)
        hidden = (jax.nn.silu(acc[w, 0]) * acc[w, 1]).astype(BF)
        hp[...] = dot(perm[...], hidden).astype(BF)
        for direction in range(2):

            def down(n, _, w=w, direction=direction):
                here = pl.ds(pl.multiple_of(n * TILE, TILE), TILE)
                there = pl.ds(pl.multiple_of(direction * HALF + n * TILE, TILE), TILE)
                product = dot(hp[...], wd[:, there]).astype(BF)
                part[w, direction, :, :, :, here] = product.reshape(2, NY, E, TILE)
                return 0

            lax.fori_loop(0, HALF // TILE, down, 0)
            pair_copy(w, direction).start()
        for direction in range(2):
            pair_copy(w, direction).wait_recv()
            to = (y + NY - 1) % NY if direction == 0 else (y + 1) % NY
            rs_send[w, direction, 0] = pair_sum(w, direction, to).astype(BF)
            reduce_copy(w, direction, 0).start()

    def ring(step, _):
        for w in range(2):
            for direction in range(2):
                to = (y + 2 * NY - 1 - step) % NY if direction == 0 else (y + 1 + step) % NY
                base = pair_sum(w, direction, to)
                reduce_copy(w, direction, step - 1).wait_recv()
                value = base + rs_recv[w, direction, step - 1].astype(F32)
                rs_send[w, direction, step] = value.astype(BF)
                reduce_copy(w, direction, step).start()
        return 0

    lax.fori_loop(1, NY - 1, ring, 0)

    for w in range(2):
        for direction in range(2):
            base = pair_sum(w, direction, y)
            reduce_copy(w, direction, NY - 2).wait_recv()
            value = base + rs_recv[w, direction, NY - 2].astype(F32)
            for j in range(HALF // LANES):
                place = direction * (HALF // LANES) + j
                stk[pl.ds(place, E, stride=T), :] = value[:, j * LANES : (j + 1) * LANES]
        ret_send[w] = stk[...].astype(BF)

        def send_back(i, _, w=w):
            peer = (e + i) % E
            pltpu.make_async_remote_copy(
                ret_send.at[w, pl.ds(pl.multiple_of(peer * T, T), T)],
                ret_recv.at[w, own_rows],
                ret_ss.at[w],
                ret_rs.at[w],
                device_id=(peer, t),
                device_id_type=MESH,
            ).start()
            return 0

        lax.fori_loop(1, E, send_back, 0)
        ret_recv[w, own_rows] = ret_send[w, own_rows]

    out = jnp.zeros((T * EXIT, LANES), F32)
    for w in range(2):
        block = ret_recv.at[w, arrivals]
        pltpu.make_async_copy(block, block, ret_rs.at[w]).wait()
        out = out + dot(c_hi[w], ret_recv[w]) + dot(c_lo[w], ret_recv[w])
    for j in range(T):
        exp_out[:, j * LANES : (j + 1) * LANES] = out[j * EXIT : (j + 1) * EXIT, :].astype(BF)

    tail.wait_send()
    head.wait_send()
    sent = carry_recv.at[pl.ds(0, E - 1)]
    pltpu.make_async_copy(sent, sent, carry_ss).wait()
    for w in range(2):
        for ref, sem in ((dsp, dsp_ss), (ret_send, ret_ss)):
            block = ref.at[w, arrivals]
            pltpu.make_async_copy(block, block, sem.at[w]).wait()
        for hop in range(H):
            for direction in range(2):
                gather_copy(w, direction, hop, halves[direction] if hop == H - 1 else whole).wait_send()
        for index in range(NY):
            sibling_copy(w, y, index).wait_send()
        for direction in range(2):
            pair_copy(w, direction).wait_send()
            for step in range(NY - 1):
                reduce_copy(w, direction, step).wait_send()


def local(
    E, T, x_path, gate_path, conv_taps, decay_gate_w, input_gate_w, decay_rate, decay_shift,
    expert_in, norm_gain, routes, route_scores, gate_weight, up_weight, down_weight,
):
    S = x_path.shape[0]
    R, D = expert_in.shape
    F = gate_weight.shape[2]
    NY, H, N, HALF = T // 2, T // 4, E * T, D // 2
    anywhere = pl.BlockSpec(memory_space=pl.ANY)
    vmem = pl.BlockSpec(memory_space=pltpu.VMEM)
    dma = pltpu.SemaphoreType.DMA
    rows = pltpu.VMEM((S, LANES), F32)
    scratch = [
        pltpu.VMEM((S, LANES), BF),
        pltpu.VMEM((S, LANES), BF),
        pltpu.VMEM((R, D), BF),
        pltpu.VMEM((D, F), BF),
        pltpu.VMEM((D, F), BF),
        pltpu.VMEM((F, D), BF),
        pltpu.VMEM((2, EXIT, LANES), BF),
        pltpu.VMEM((S + 2 * EXIT, LANES), F32),
        rows,
        rows,
        rows,
        rows,
        rows,
        rows,
        rows,
        pltpu.VMEM((4, 8, LANES), F32),
        pltpu.VMEM((8, LANES), F32),
        pltpu.VMEM((E, 8, LANES), F32),
        pltpu.VMEM((2, N, LANES), BF),
        pltpu.VMEM((2, NY, 2, N, LANES), BF),
        pltpu.VMEM((2, 2, N, F), F32),
        pltpu.VMEM((N, N), BF),
        pltpu.VMEM((N, F), BF),
        pltpu.VMEM((2, 2, 2, NY, E, HALF), BF),
        pltpu.VMEM((2, 2, NY, E, HALF), BF),
        pltpu.VMEM((2, 2, NY - 1, E, HALF), BF),
        pltpu.VMEM((2, 2, NY - 1, E, HALF), BF),
        pltpu.VMEM((N, LANES), F32),
        pltpu.VMEM((2, N, LANES), BF),
        pltpu.VMEM((2, N, LANES), BF),
        pltpu.VMEM((2, T * EXIT, N), BF),
        pltpu.VMEM((2, T * EXIT, N), BF),
        dma((6,)),
        dma((2,)),
        dma((2,)),
        dma,
        dma,
        dma((2,)),
        dma((2,)),
        dma((2, 2, H)),
        dma((2, 2, H)),
        dma((2, NY)),
        dma((2, NY)),
        dma((2, 2)),
        dma((2, 2)),
        dma((2, 2, NY - 1)),
        dma((2, 2, NY - 1)),
        dma((2,)),
        dma((2,)),
    ]
    return pl.pallas_call(
        functools.partial(layer, E, T),
        out_shape=(
            jax.ShapeDtypeStruct((S, LANES), BF),
            jax.ShapeDtypeStruct((EXIT, D), BF),
        ),
        in_specs=[anywhere] * 6 + [vmem] * 9,
        out_specs=(vmem, vmem),
        scratch_shapes=scratch,
        compiler_params=pltpu.CompilerParams(
            collective_id=0, has_side_effects=True, vmem_limit_bytes=60 * 1024 * 1024
        ),
        name="layer",
    )(
        x_path,
        gate_path,
        expert_in,
        gate_weight.reshape(D, F),
        up_weight.reshape(D, F),
        down_weight.reshape(F, D),
        conv_taps,
        decay_gate_w,
        input_gate_w,
        decay_rate,
        decay_shift.reshape(8, S // 8),
        norm_gain.reshape(D // LANES, LANES),
        routes,
        routes.T,
        route_scores,
    )


def solution(mesh):
    in_specs = (
        P("ep", "tp"),
        P("ep", "tp"),
        P(None, "tp"),
        P(None, "tp", None, None),
        P(None, "tp", None, None),
        P(None, "tp"),
        P("ep", "tp"),
        P("ep", None),
        P(),
        P("ep", None),
        P("ep", None),
        P("ep", None, "tp"),
        P("ep", None, "tp"),
        P("ep", "tp", None),
    )
    out_specs = (P("ep", "tp"), P(("ep", "tp"), None))
    step = functools.partial(local, mesh.shape["ep"], mesh.shape["tp"])
    return jax.shard_map(step, mesh=mesh, in_specs=in_specs, out_specs=out_specs, check_vma=False)
```

```python
import functools

import jax
import jax.numpy as jnp
from jax import lax
from jax.experimental import pallas as pl
from jax.experimental.pallas import tpu as pltpu
from jax.sharding import PartitionSpec as P

BF = jnp.bfloat16
F32 = jnp.float32
I32 = jnp.int32
MESH = pl.DeviceIdType.MESH
EPSILON = 1e-06
LANES = 128
EXIT = 16


def log2(n):
    return n.bit_length() - 1


def iota(shape, dim):
    return lax.broadcasted_iota(I32, shape, dim)


def shr(x, n):
    return lax.shift_right_logical(x, jnp.full(x.shape, n, I32))


def dot(a, b):
    return jnp.dot(a, b, preferred_element_type=F32)


def one_hot(mask):
    return jnp.where(mask, 1.0, 0.0).astype(BF)


def one_minus_square(log_a, a):
    z = 2.0 * log_a
    series = 1.0 + z * (1 / 2 + z * (1 / 6 + z * (1 / 24 + z * (1 / 120 + z * (1 / 720)))))
    return jnp.where(z > -0.25, -z * series, 1.0 - a * a)


def layer(
    E,
    T,
    x_hbm,
    gate_hbm,
    ein_hbm,
    wg_hbm,
    wu_hbm,
    wd_hbm,
    taps,
    dgw,
    igw,
    rate,
    shift,
    gain,
    routes_t,
    scores_t,
    rec_out,
    exp_out,
    xraw,
    gatev,
    ein,
    wg,
    wu,
    wd,
    halo,
    xpad,
    sh,
    cperm,
    af,
    bf,
    ab,
    bb,
    ynat,
    seg,
    carry_send,
    carry_recv,
    dsp,
    xb,
    acc,
    perm,
    hp,
    part,
    sibp,
    rs_send,
    rs_recv,
    stk,
    ret_send,
    ret_recv,
    c_hi,
    c_lo,
    load_sem,
    halo_ss,
    halo_rs,
    carry_ss,
    carry_rs,
    dsp_ss,
    dsp_rs,
    ag_ss,
    ag_rs,
    sib_ss,
    sib_rs,
    sp_ss,
    sp_rs,
    rs_ss,
    rs_rs,
    ret_ss,
    ret_rs,
):
    NY, H = T // 2, T // 4
    S = xraw.shape[0]
    NS = S // 8
    R, D = ein.shape
    F = wg.shape[1]
    HALF = D // 2
    N = E * T
    lT, lE, lNY = log2(T), log2(E), log2(NY)

    e = lax.axis_index("ep")
    t = lax.axis_index("tp")
    y = t // 2
    c = t % 2
    sib_t = y * 2 + (1 - c)
    right_t = ((y + 1) % NY) * 2 + c
    left_t = ((y + NY - 1) % NY) * 2 + c
    ep_next = (e + 1) % E
    ep_prev = (e + E - 1) % E

    loads = [
        pltpu.make_async_copy(src, dst, load_sem.at[i])
        for i, (src, dst) in enumerate(
            ((ein_hbm, ein), (x_hbm, xraw), (wg_hbm, wg), (wu_hbm, wu), (gate_hbm, gatev), (wd_hbm, wd))
        )
    ]
    for load in loads:
        load.start()

    barrier = pltpu.get_barrier_semaphore()

    def greet(i, _):
        pl.semaphore_signal(barrier, inc=1, device_id=((e + i) % E, t), device_id_type=MESH)
        return 0

    lax.fori_loop(1, E, greet, 0)
    for peer in (sib_t, right_t, left_t):
        pl.semaphore_signal(barrier, inc=1, device_id=(e, peer), device_id_type=MESH)

    ids = iota((E, R), 0)
    first_t = routes_t[0:1, :] == ids
    second_t = routes_t[1:2, :] == ids
    named_t = one_hot(first_t | second_t)
    rr, rc = iota((R, R), 0), iota((R, R), 1)
    earlier_t = one_hot((shr(rr, 4) == shr(rc, 4)) & (rr < rc))
    rank_t = dot(named_t, earlier_t)
    loads[0].wait()
    total = jnp.zeros((R, LANES), F32)
    for j in range(D // LANES):
        tile = ein[:, j * LANES : (j + 1) * LANES].astype(F32)
        total = total + tile * tile
    scale = lax.rsqrt(jnp.sum(total, axis=1, keepdims=True) * (1.0 / D) + EPSILON)
    own_columns = pl.ds(pl.multiple_of(t * LANES, LANES), LANES)
    normed = (ein[:, own_columns].astype(F32) * scale * gain[pl.ds(t, 1), :]).astype(BF)
    spread = one_hot(shr(iota((N, E), 0), lT) == iota((N, E), 1))
    in_block = (iota((N, R), 0) & (T - 1)) == shr(iota((N, R), 1), 4)
    for w in range(2):
        chosen = jnp.where(rank_t == float(w), named_t.astype(F32), 0.0).astype(BF)
        selector = jnp.where(in_block, dot(spread, chosen), 0.0).astype(BF)
        dsp[w] = dot(selector, normed).astype(BF)

    loads[1].wait()
    pl.semaphore_wait(barrier, E + 2)

    tail = pltpu.make_async_remote_copy(
        xraw.at[pl.ds(S - EXIT, EXIT)], halo.at[0], halo_ss.at[0], halo_rs.at[0],
        device_id=(ep_next, t), device_id_type=MESH,
    )
    head = pltpu.make_async_remote_copy(
        xraw.at[pl.ds(0, EXIT)], halo.at[1], halo_ss.at[1], halo_rs.at[1],
        device_id=(ep_prev, t), device_id_type=MESH,
    )
    tail.start()
    head.start()

    own_rows = pl.ds(pl.multiple_of(e * T, T), T)
    for w in range(2):

        def send(i, _, w=w):
            peer = (e + i) % E
            pltpu.make_async_remote_copy(
                dsp.at[w, pl.ds(pl.multiple_of(peer * T, T), T)],
                xb.at[w, y, c, own_rows],
                dsp_ss.at[w],
                dsp_rs.at[w],
                device_id=(peer, t),
                device_id_type=MESH,
            ).start()
            return 0

        lax.fori_loop(1, E, send, 0)
        xb[w, y, c, own_rows] = dsp[w, own_rows]

    n0, n1 = iota((N, N), 0), iota((N, N), 1)
    perm_block = (shr(n0, lE) & (NY - 1)) * 2 + shr(n0, lE + lNY)
    perm[...] = one_hot((shr(n1, lT) == (n0 & (E - 1))) & ((n1 & (T - 1)) == perm_block))

    shares_t = scores_t[...] / (scores_t[0:1, :] + scores_t[1:2, :])
    share_of = jnp.where(first_t, shares_t[0:1, :], 0.0) + jnp.where(second_t, shares_t[1:2, :], 0.0)
    own_row = t * EXIT + (iota((T * EXIT, R), 0) & (EXIT - 1))
    rows_out = one_hot(own_row == iota((T * EXIT, R), 1))
    columns_out = one_hot(iota((E, N), 0) == shr(iota((E, N), 1), lT))
    same_tile = shr(iota((T * EXIT, N), 0), 4) == (iota((T * EXIT, N), 1) & (T - 1))
    for w in range(2):
        weight = jnp.where(rank_t == float(w), share_of, 0.0)
        high = weight.astype(BF)
        low = (weight - high.astype(F32)).astype(BF)
        for piece, table in ((high, c_hi), (low, c_lo)):
            picked = lax.dot_general(rows_out, piece, (((1,), (1,)), ((), ())), preferred_element_type=F32)
            wide = dot(picked.astype(BF), columns_out)
            table[w] = jnp.where(same_tile, wide, 0.0).astype(BF)

    xpad[pl.ds(EXIT, S), :] = xraw[...].astype(F32)
    for s in range(NS):
        sh[pl.ds(s * 8, 8), :] = jnp.broadcast_to(shift[:, s : s + 1], (8, LANES))
    tail.wait_recv()
    head.wait_recv()
    xpad[pl.ds(0, EXIT), :] = jnp.where(e > 0, halo[0].astype(F32), 0.0)
    xpad[pl.ds(EXIT + S, EXIT), :] = jnp.where(e < E - 1, halo[1].astype(F32), 0.0)

    def strided(s):
        return xpad[pl.ds(EXIT + s, 8, stride=NS), :]

    tap = [taps[k : k + 1, :] for k in range(4)]

    def conv(s, held):
        v0, v1, v2 = held
        v3 = strided(s + 1)
        value = v0 * tap[0] + v1 * tap[1] + v2 * tap[2] + v3 * tap[3]
        cperm[pl.ds(pl.multiple_of(s * 8, 8), 8), :] = value.astype(BF).astype(F32)
        return v1, v2, v3

    lax.fori_loop(0, NS, conv, (strided(-2), strided(-1), strided(0)), unroll=8)

    CH = min(128, S)

    def gates(i, _):
        rows = pl.ds(pl.multiple_of(i * CH, CH), CH)
        value = cperm[rows, :]
        value_b = value.astype(BF)
        shift_here = sh[rows, :]
        for d, (a_ref, b_ref) in enumerate(((af, bf), (ab, bb))):
            decay_gate = jax.nn.sigmoid(dot(value_b, dgw[d, 0]))
            input_gate = jax.nn.sigmoid(dot(value_b, igw[d, 0]))
            log_decay = -8.0 * decay_gate * rate[d : d + 1, :] + shift_here
            decay = jnp.exp(log_decay)
            rest = one_minus_square(log_decay, decay)
            root = rest * lax.rsqrt(jnp.maximum(rest, 1e-37))
            a_ref[rows, :] = decay
            b_ref[rows, :] = root * input_gate * value
        return 0

    lax.fori_loop(0, S // CH, gates, 0)

    def at(s):
        return pl.ds(pl.multiple_of(s * 8, 8), 8)

    def summing(s, held):
        hf, pf, hb, pb = held
        a, b = af[at(s), :], bf[at(s), :]
        a2, b2 = ab[at(NS - 1 - s), :], bb[at(NS - 1 - s), :]
        return a * hf + b, a * pf, a2 * hb + b2, a2 * pb

    zero, one = jnp.zeros((8, LANES), F32), jnp.ones((8, LANES), F32)
    hf, pf, hb, pb = lax.fori_loop(0, NS, summing, (zero, one, zero, one), unroll=8)
    for k, value in enumerate((pf, hf, pb, hb)):
        seg[k] = value

    def segment(k, g):
        return seg[k, g : g + 1, :]

    ones = jnp.ones((1, LANES), F32)
    fa, fb, ba, bb_ = ones, ones * 0.0, ones, ones * 0.0
    for g in range(8):
        fa, fb = segment(0, g) * fa, segment(0, g) * fb + segment(1, g)
        ba, bb_ = segment(2, 7 - g) * ba, segment(2, 7 - g) * bb_ + segment(3, 7 - g)
    ahead = jnp.concatenate([fa, fb], axis=0)
    behind = jnp.concatenate([ba, bb_], axis=0)
    carry_send[0] = ahead
    carry_send[1] = behind
    carry_recv[e] = ahead

    def send_carry(i, _):
        peer = (e + i) % E
        pltpu.make_async_remote_copy(
            carry_send.at[(peer < e).astype(I32)], carry_recv.at[e], carry_ss, carry_rs,
            device_id=(peer, t), device_id_type=MESH,
        ).start()
        return 0

    lax.fori_loop(1, E, send_carry, 0)

    def gather_copy(w, direction, hop, rows):
        source = (y + NY - hop) % NY if direction == 0 else (y + hop) % NY
        block = xb.at[w, source, c, rows]
        return pltpu.make_async_remote_copy(
            block, block, ag_ss.at[w, direction, hop], ag_rs.at[w, direction, hop],
            device_id=(e, right_t if direction == 0 else left_t), device_id_type=MESH,
        )

    def arrived_gather(w, direction, hop, rows):
        source = (y + 2 * NY - hop - 1) % NY if direction == 0 else (y + hop + 1) % NY
        block = xb.at[w, source, c, rows]
        pltpu.make_async_copy(block, block, ag_rs.at[w, direction, hop]).wait()

    whole = pl.ds(0, N)
    halves = (pl.ds(0, N // 2), pl.ds(N // 2, N // 2))

    def forward(w, direction, hop):
        if isinstance(hop, int):
            gather_copy(w, direction, hop, halves[direction] if hop == H - 1 else whole).start()

    def sibling_copy(w, source, index):
        block = xb.at[w, source, c]
        return pltpu.make_async_remote_copy(
            block, block, sib_ss.at[w, index], sib_rs.at[w, index],
            device_id=(e, sib_t), device_id_type=MESH,
        )

    def sibling_arrived(w, source, index):
        block = xb.at[w, source, 1 - c]
        pltpu.make_async_copy(block, block, sib_rs.at[w, index]).wait()

    def multiply(w, source, fresh):
        rows = jnp.concatenate([xb[w, source, 0], xb[w, source, 1]], axis=1)
        depth = pl.ds(pl.multiple_of(source * 2 * LANES, 2 * LANES), 2 * LANES)
        for k, weight in enumerate((wg, wu)):
            product = dot(rows, weight[depth, :])
            if fresh:
                acc[w, k] = product
            else:
                acc[w, k] += product

    arrivals = pl.ds(0, (E - 1) * T)
    for w in range(2):
        block = xb.at[w, y, c, arrivals]
        pltpu.make_async_copy(block, block, dsp_rs.at[w]).wait()
        forward(w, 0, 0)
        forward(w, 1, 0)
        sibling_copy(w, y, 0).start()

    loads[2].wait()
    loads[3].wait()
    for w in range(2):
        sibling_arrived(w, y, 0)
        multiply(w, y, True)

    for hop in range(1, H):
        rights, lefts = (y + NY - hop) % NY, (y + hop) % NY
        for w in range(2):
            arrived_gather(w, 0, hop - 1, whole)
            forward(w, 0, hop)
            arrived_gather(w, 1, hop - 1, whole)
            forward(w, 1, hop)
            sibling_copy(w, rights, 2 * hop - 1).start()
            sibling_copy(w, lefts, 2 * hop).start()
        for w in range(2):
            sibling_arrived(w, rights, 2 * hop - 1)
            multiply(w, rights, False)
            sibling_arrived(w, lefts, 2 * hop)
            multiply(w, lefts, False)

    far = (y + H) % NY

    def reduce_copy(w, direction, step):
        return pltpu.make_async_remote_copy(
            rs_send.at[w, direction, step], rs_recv.at[w, direction, step],
            rs_ss.at[w, direction, step], rs_rs.at[w, direction, step],
            device_id=(e, right_t if direction == 0 else left_t), device_id_type=MESH,
        )

    def pair_copy(w, direction):
        return pltpu.make_async_remote_copy(
            part.at[w, direction, 1 - c], sibp.at[w, direction],
            sp_ss.at[w, direction], sp_rs.at[w, direction],
            device_id=(e, sib_t), device_id_type=MESH,
        )

    def pair_sum(w, direction, to):
        return part[w, direction, c, to].astype(F32) + sibp[w, direction, to].astype(F32)

    loads[5].wait()
    TILE = min(256, HALF)
    for w in range(2):
        arrived_gather(w, 0, H - 1, halves[0])
        arrived_gather(w, 1, H - 1, halves[1])
        sibling_copy(w, far, NY - 1).start()
        sibling_arrived(w, far, NY - 1)
        multiply(w, far, False)
        hidden = (jax.nn.silu(acc[w, 0]) * acc[w, 1]).astype(BF)
        hp[...] = dot(perm[...], hidden).astype(BF)
        for direction in range(2):

            def down(n, _, w=w, direction=direction):
                here = pl.ds(pl.multiple_of(n * TILE, TILE), TILE)
                there = pl.ds(pl.multiple_of(direction * HALF + n * TILE, TILE), TILE)
                product = dot(hp[...], wd[:, there]).astype(BF)
                part[w, direction, :, :, :, here] = product.reshape(2, NY, E, TILE)
                return 0

            lax.fori_loop(0, HALF // TILE, down, 0)
            pair_copy(w, direction).start()
        for direction in range(2):
            pair_copy(w, direction).wait_recv()
            to = (y + NY - 1) % NY if direction == 0 else (y + 1) % NY
            rs_send[w, direction, 0] = pair_sum(w, direction, to).astype(BF)
            reduce_copy(w, direction, 0).start()

    def ring(step, _):
        for w in range(2):
            for direction in range(2):
                to = (y + 2 * NY - 1 - step) % NY if direction == 0 else (y + 1 + step) % NY
                base = pair_sum(w, direction, to)
                reduce_copy(w, direction, step - 1).wait_recv()
                value = base + rs_recv[w, direction, step - 1].astype(F32)
                rs_send[w, direction, step] = value.astype(BF)
                reduce_copy(w, direction, step).start()
        return 0

    lax.fori_loop(1, NY - 1, ring, 0)

    for w in range(2):
        for direction in range(2):
            base = pair_sum(w, direction, y)
            reduce_copy(w, direction, NY - 2).wait_recv()
            value = base + rs_recv[w, direction, NY - 2].astype(F32)
            for j in range(HALF // LANES):
                place = direction * (HALF // LANES) + j
                stk[pl.ds(place, E, stride=T), :] = value[:, j * LANES : (j + 1) * LANES]
        ret_send[w] = stk[...].astype(BF)

        def send_back(i, _, w=w):
            peer = (e + i) % E
            pltpu.make_async_remote_copy(
                ret_send.at[w, pl.ds(pl.multiple_of(peer * T, T), T)],
                ret_recv.at[w, own_rows],
                ret_ss.at[w],
                ret_rs.at[w],
                device_id=(peer, t),
                device_id_type=MESH,
            ).start()
            return 0

        lax.fori_loop(1, E, send_back, 0)
        ret_recv[w, own_rows] = ret_send[w, own_rows]

    pltpu.make_async_copy(
        carry_recv.at[pl.ds(0, E - 1)], carry_recv.at[pl.ds(0, E - 1)], carry_rs
    ).wait()

    def fold(i, held):
        f, b = held
        one_way = carry_recv[i]
        j = E - 1 - i
        other = carry_recv[j]
        f = jnp.where(i < e, one_way[0:1] * f + one_way[1:2], f)
        b = jnp.where(j > e, other[0:1] * b + other[1:2], b)
        return f, b

    f, b = lax.fori_loop(0, E, fold, (ones * 0.0, ones * 0.0))
    f_rows, b_rows = [f], [b]
    for g in range(7):
        f_rows.append(segment(0, g) * f_rows[-1] + segment(1, g))
        b_rows.insert(0, segment(2, 7 - g) * b_rows[0] + segment(3, 7 - g))
    f_in, b_in = jnp.concatenate(f_rows, axis=0), jnp.concatenate(b_rows, axis=0)

    def states(s, held):
        hf, hb = held
        r = NS - 1 - s
        hf = af[at(s), :] * hf + bf[at(s), :]
        hb = ab[at(r), :] * hb + bb[at(r), :]
        bf[at(s), :] = hf
        bb[at(r), :] = hb
        return hf, hb

    lax.fori_loop(0, NS, states, (f_in, b_in), unroll=8)

    def natural(s, _):
        ynat[pl.ds(s, 8, stride=NS), :] = bf[at(s), :] + bb[at(s), :]
        return 0

    lax.fori_loop(0, NS, natural, 0, unroll=8)
    loads[4].wait()

    def finish(i, _):
        rows = pl.ds(pl.multiple_of(i * CH, CH), CH)
        rec_out[rows, :] = (ynat[rows, :] * jax.nn.gelu(gatev[rows, :].astype(F32))).astype(BF)
        return 0

    lax.fori_loop(0, S // CH, finish, 0)

    out = jnp.zeros((T * EXIT, LANES), F32)
    for w in range(2):
        block = ret_recv.at[w, arrivals]
        pltpu.make_async_copy(block, block, ret_rs.at[w]).wait()
        out = out + dot(c_hi[w], ret_recv[w]) + dot(c_lo[w], ret_recv[w])
    for j in range(T):
        exp_out[:, j * LANES : (j + 1) * LANES] = out[j * EXIT : (j + 1) * EXIT, :].astype(BF)

    tail.wait_send()
    head.wait_send()
    sent = carry_recv.at[pl.ds(0, E - 1)]
    pltpu.make_async_copy(sent, sent, carry_ss).wait()
    for w in range(2):
        for ref, sem in ((dsp, dsp_ss), (ret_send, ret_ss)):
            block = ref.at[w, arrivals]
            pltpu.make_async_copy(block, block, sem.at[w]).wait()
        for hop in range(H):
            for direction in range(2):
                gather_copy(w, direction, hop, halves[direction] if hop == H - 1 else whole).wait_send()
        for index in range(NY):
            sibling_copy(w, y, index).wait_send()
        for direction in range(2):
            pair_copy(w, direction).wait_send()
            for step in range(NY - 1):
                reduce_copy(w, direction, step).wait_send()


def local(
    E, T, x_path, gate_path, conv_taps, decay_gate_w, input_gate_w, decay_rate, decay_shift,
    expert_in, norm_gain, routes, route_scores, gate_weight, up_weight, down_weight,
):
    S = x_path.shape[0]
    R, D = expert_in.shape
    F = gate_weight.shape[2]
    NY, H, N, HALF = T // 2, T // 4, E * T, D // 2
    anywhere = pl.BlockSpec(memory_space=pl.ANY)
    vmem = pl.BlockSpec(memory_space=pltpu.VMEM)
    dma = pltpu.SemaphoreType.DMA
    rows = pltpu.VMEM((S, LANES), F32)
    scratch = [
        pltpu.VMEM((S, LANES), BF),
        pltpu.VMEM((S, LANES), BF),
        pltpu.VMEM((R, D), BF),
        pltpu.VMEM((D, F), BF),
        pltpu.VMEM((D, F), BF),
        pltpu.VMEM((F, D), BF),
        pltpu.VMEM((2, EXIT, LANES), BF),
        pltpu.VMEM((S + 2 * EXIT, LANES), F32),
        rows,
        rows,
        rows,
        rows,
        rows,
        rows,
        rows,
        pltpu.VMEM((4, 8, LANES), F32),
        pltpu.VMEM((2, 2, LANES), F32),
        pltpu.VMEM((E, 2, LANES), F32),
        pltpu.VMEM((2, N, LANES), BF),
        pltpu.VMEM((2, NY, 2, N, LANES), BF),
        pltpu.VMEM((2, 2, N, F), F32),
        pltpu.VMEM((N, N), BF),
        pltpu.VMEM((N, F), BF),
        pltpu.VMEM((2, 2, 2, NY, E, HALF), BF),
        pltpu.VMEM((2, 2, NY, E, HALF), BF),
        pltpu.VMEM((2, 2, NY - 1, E, HALF), BF),
        pltpu.VMEM((2, 2, NY - 1, E, HALF), BF),
        pltpu.VMEM((N, LANES), F32),
        pltpu.VMEM((2, N, LANES), BF),
        pltpu.VMEM((2, N, LANES), BF),
        pltpu.VMEM((2, T * EXIT, N), BF),
        pltpu.VMEM((2, T * EXIT, N), BF),
        dma((6,)),
        dma((2,)),
        dma((2,)),
        dma,
        dma,
        dma((2,)),
        dma((2,)),
        dma((2, 2, H)),
        dma((2, 2, H)),
        dma((2, NY)),
        dma((2, NY)),
        dma((2, 2)),
        dma((2, 2)),
        dma((2, 2, NY - 1)),
        dma((2, 2, NY - 1)),
        dma((2,)),
        dma((2,)),
    ]
    return pl.pallas_call(
        functools.partial(layer, E, T),
        out_shape=(
            jax.ShapeDtypeStruct((S, LANES), BF),
            jax.ShapeDtypeStruct((EXIT, D), BF),
        ),
        in_specs=[anywhere] * 6 + [vmem] * 8,
        out_specs=(vmem, vmem),
        scratch_shapes=scratch,
        compiler_params=pltpu.CompilerParams(
            collective_id=0, has_side_effects=True, vmem_limit_bytes=60 * 1024 * 1024
        ),
        name="layer",
    )(
        x_path,
        gate_path,
        expert_in,
        gate_weight.reshape(D, F),
        up_weight.reshape(D, F),
        down_weight.reshape(F, D),
        conv_taps,
        decay_gate_w,
        input_gate_w,
        decay_rate,
        decay_shift.reshape(8, S // 8),
        norm_gain.reshape(D // LANES, LANES),
        routes.T,
        route_scores.T,
    )


def solution(mesh):
    in_specs = (
        P("ep", "tp"),
        P("ep", "tp"),
        P(None, "tp"),
        P(None, "tp", None, None),
        P(None, "tp", None, None),
        P(None, "tp"),
        P("ep", "tp"),
        P("ep", None),
        P(),
        P("ep", None),
        P("ep", None),
        P("ep", None, "tp"),
        P("ep", None, "tp"),
        P("ep", "tp", None),
    )
    out_specs = (P("ep", "tp"), P(("ep", "tp"), None))
    step = functools.partial(local, mesh.shape["ep"], mesh.shape["tp"])
    return jax.shard_map(step, mesh=mesh, in_specs=in_specs, out_specs=out_specs, check_vma=False)
```

```python
import functools

import jax
import jax.numpy as jnp
from jax import lax
from jax.experimental import pallas as pl
from jax.experimental.pallas import tpu as pltpu
from jax.sharding import PartitionSpec as P

BF = jnp.bfloat16
F32 = jnp.float32
I32 = jnp.int32
MESH = pl.DeviceIdType.MESH
EPSILON = 1e-06
LANES = 128
EXIT = 16


def log2(n):
    return n.bit_length() - 1


def iota(shape, dim):
    return lax.broadcasted_iota(I32, shape, dim)


def shr(x, n):
    return lax.shift_right_logical(x, jnp.full(x.shape, n, I32))


def dot(a, b):
    return jnp.dot(a, b, preferred_element_type=F32)


def one_hot(mask):
    return jnp.where(mask, 1.0, 0.0).astype(BF)


def one_minus_square(log_a, a):
    z = 2.0 * log_a
    series = 1.0 + z * (1 / 2 + z * (1 / 6 + z * (1 / 24 + z * (1 / 120 + z * (1 / 720)))))
    return jnp.where(z > -0.25, -z * series, 1.0 - a * a)


def plane(E):
    X = 4 if E >= 32 else min(2, E)
    Z = E // X
    near = (
        [(0, 0), (0, 1), (0, 3), (1, 0), (7, 0), (1, 1), (7, 3), (0, 2)]
        + [(1, 3), (7, 1), (1, 2), (7, 2), (2, 0), (6, 0), (2, 1), (6, 3)]
        if E == 32
        else [(i // X, i % X) for i in range(E // 2)]
    )
    rest = [(z, x) for z in range(Z) for x in range(X) if (z, x) not in near]
    rest.sort(key=lambda p: -(min(p[0], Z - p[0]) + min(p[1], X - p[1])))
    return X, Z, near + rest


def layer(
    E,
    T,
    x_hbm,
    gate_hbm,
    ein_hbm,
    wg_hbm,
    wu_hbm,
    wd_hbm,
    taps,
    dgw,
    igw,
    rate,
    shift,
    gain,
    routes_t,
    scores_t,
    rec_out,
    exp_out,
    xraw,
    gatev,
    ein,
    wg,
    wu,
    wd,
    halo,
    xpad,
    sh,
    cperm,
    af,
    bf,
    ab,
    bb,
    ynat,
    seg,
    carry_send,
    carry_recv,
    named_as,
    far_select,
    near_select,
    normed,
    dsp,
    near_send,
    xb,
    xn,
    acc,
    perm,
    hp,
    part,
    pair,
    sums,
    came,
    stk,
    back,
    ret_recv,
    c_hi,
    c_lo,
    load_sem,
    halo_ss,
    halo_rs,
    carry_ss,
    carry_rs,
    dsp_ss,
    dsp_rs,
    near_ss,
    near_rs,
    mate_ss,
    mate_rs,
    ag_ss,
    ag_rs,
    sib_ss,
    sib_rs,
    sp_ss,
    sp_rs,
    rs_ss,
    rs_rs,
    ret_ss,
    ret_rs,
):
    NY, H, K, G = T // 2, T // 4, E // 2, E // 4
    S = xraw.shape[0]
    NS = S // 8
    R, D = ein.shape
    F = wg.shape[1]
    HALF = D // 2
    N, M, GT = E * T, K * T, G * T
    lT, lNY = log2(T), log2(NY)
    X, Z, slots = plane(E)

    e = lax.axis_index("ep")
    t = lax.axis_index("tp")
    y = t // 2
    c = t % 2
    sib_t = y * 2 + (1 - c)
    right_t = ((y + 1) % NY) * 2 + c
    left_t = ((y + NY - 1) % NY) * 2 + c
    ep_next = (e + 1) % E
    ep_prev = (e + E - 1) % E
    ez, ex = e // X, e % X

    def source_of(slot):
        dz, dx = slots[slot]
        return ((ez + dz) % Z) * X + (ex + dx) % X

    def target_of(slot):
        dz, dx = slots[slot]
        return ((ez + Z - dz) % Z) * X + (ex + X - dx) % X

    loads = [
        pltpu.make_async_copy(src, dst, load_sem.at[i])
        for i, (src, dst) in enumerate(
            ((ein_hbm, ein), (x_hbm, xraw), (wg_hbm, wg), (wu_hbm, wu), (gate_hbm, gatev), (wd_hbm, wd))
        )
    ]
    for load in loads:
        load.start()

    barrier = pltpu.get_barrier_semaphore()

    def greet(i, _):
        pl.semaphore_signal(barrier, inc=1, device_id=((e + i) % E, t), device_id_type=MESH)
        return 0

    lax.fori_loop(1, E, greet, 0)
    for peer in (sib_t, right_t, left_t):
        pl.semaphore_signal(barrier, inc=1, device_id=(e, peer), device_id_type=MESH)

    ids = iota((E, R), 0)
    first_t = routes_t[0:1, :] == ids
    second_t = routes_t[1:2, :] == ids
    named_t = one_hot(first_t | second_t)
    rr, rc = iota((R, R), 0), iota((R, R), 1)
    earlier_t = one_hot((shr(rr, 4) == shr(rc, 4)) & (rr < rc))
    rank_t = dot(named_t, earlier_t)
    for w in range(2):
        named_as[w] = jnp.where(rank_t == float(w), named_t.astype(F32), 0.0)
    in_block = iota((T, R), 0) == shr(iota((T, R), 1), 4)

    def selector(w, slot):
        named = named_as[w, pl.ds(target_of(slot), 1), :]
        return jnp.where(in_block, jnp.broadcast_to(named, (T, R)), 0.0).astype(BF)

    for w in range(2):
        for j in range(K):
            far_select[w, j * T : (j + 1) * T, :] = selector(w, K + j)
    loads[0].wait()
    total = jnp.zeros((R, LANES), F32)
    for j in range(D // LANES):
        tile = ein[:, j * LANES : (j + 1) * LANES].astype(F32)
        total = total + tile * tile
    scale = lax.rsqrt(jnp.sum(total, axis=1, keepdims=True) * (1.0 / D) + EPSILON)

    def normed_tile(j):
        columns = pl.ds(pl.multiple_of(j * LANES, LANES), LANES)
        return (ein[:, columns].astype(F32) * scale * gain[pl.ds(j, 1), :]).astype(BF)

    own_normed = normed_tile(t)
    for w in range(2):
        dsp[w] = dot(far_select[w], own_normed).astype(BF)

    loads[1].wait()
    pl.semaphore_wait(barrier, E + 2)

    tail = pltpu.make_async_remote_copy(
        xraw.at[pl.ds(S - EXIT, EXIT)], halo.at[0], halo_ss.at[0], halo_rs.at[0],
        device_id=(ep_next, t), device_id_type=MESH,
    )
    head = pltpu.make_async_remote_copy(
        xraw.at[pl.ds(0, EXIT)], halo.at[1], halo_ss.at[1], halo_rs.at[1],
        device_id=(ep_prev, t), device_id_type=MESH,
    )
    tail.start()
    head.start()

    own_rows = pl.ds(pl.multiple_of(e * T, T), T)
    for w in range(2):
        for j in range(K):
            rows = pl.ds(j * T, T)
            pltpu.make_async_remote_copy(
                dsp.at[w, rows], xb.at[w, y, c, rows], dsp_ss.at[w], dsp_rs.at[w],
                device_id=(target_of(K + j), t), device_id_type=MESH,
            ).start()

    for j in range(D // LANES):
        normed[:, j * LANES : (j + 1) * LANES] = normed_tile(j)
    for k in range(K):
        near_select[k * T : (k + 1) * T, :] = selector(c, k)
    near_send[...] = dot(near_select[...], normed[...]).astype(BF).reshape(2, GT, D)
    for k in range(K):
        g, rows = k // G, pl.ds(k % G * T, T)
        if k == 0:
            xn[g, c, rows, :] = near_send[g, rows, :]
            continue
        pltpu.make_async_remote_copy(
            near_send.at[g, rows], xn.at[g, c, rows], near_ss.at[g], near_rs.at[g],
            device_id=(target_of(k), t), device_id_type=MESH,
        ).start()

    n0, n1 = iota((M, M), 0), iota((M, M), 1)
    perm_block = (shr(n0, log2(K)) & (NY - 1)) * 2 + shr(n0, log2(K) + lNY)
    perm[...] = one_hot((shr(n1, lT) == (n0 & (K - 1))) & ((n1 & (T - 1)) == perm_block))

    xpad[pl.ds(EXIT, S), :] = xraw[...].astype(F32)
    for s in range(NS):
        sh[pl.ds(s * 8, 8), :] = jnp.broadcast_to(shift[:, s : s + 1], (8, LANES))
    tail.wait_recv()
    head.wait_recv()
    xpad[pl.ds(0, EXIT), :] = jnp.where(e > 0, halo[0].astype(F32), 0.0)
    xpad[pl.ds(EXIT + S, EXIT), :] = jnp.where(e < E - 1, halo[1].astype(F32), 0.0)

    def strided(s):
        return xpad[pl.ds(EXIT + s, 8, stride=NS), :]

    tap = [taps[k : k + 1, :] for k in range(4)]

    def conv(s, held):
        v0, v1, v2 = held
        v3 = strided(s + 1)
        value = v0 * tap[0] + v1 * tap[1] + v2 * tap[2] + v3 * tap[3]
        cperm[pl.ds(pl.multiple_of(s * 8, 8), 8), :] = value.astype(BF).astype(F32)
        return v1, v2, v3

    lax.fori_loop(0, NS, conv, (strided(-2), strided(-1), strided(0)), unroll=8)

    CH = min(128, S)

    def gates(i, _):
        rows = pl.ds(pl.multiple_of(i * CH, CH), CH)
        value = cperm[rows, :]
        value_b = value.astype(BF)
        shift_here = sh[rows, :]
        for d, (a_ref, b_ref) in enumerate(((af, bf), (ab, bb))):
            decay_gate = jax.nn.sigmoid(dot(value_b, dgw[d, 0]))
            input_gate = jax.nn.sigmoid(dot(value_b, igw[d, 0]))
            log_decay = -8.0 * decay_gate * rate[d : d + 1, :] + shift_here
            decay = jnp.exp(log_decay)
            rest = one_minus_square(log_decay, decay)
            root = rest * lax.rsqrt(jnp.maximum(rest, 1e-37))
            a_ref[rows, :] = decay
            b_ref[rows, :] = root * input_gate * value
        return 0

    lax.fori_loop(0, S // CH, gates, 0)

    def gather_copy(w, direction, hop):
        source = (y + NY - hop) % NY if direction == 0 else (y + hop) % NY
        block = xb.at[w, source, c, span(direction, hop)]
        return pltpu.make_async_remote_copy(
            block, block, ag_ss.at[w, direction, hop], ag_rs.at[w, direction, hop],
            device_id=(e, right_t if direction == 0 else left_t), device_id_type=MESH,
        )

    def span(direction, hop):
        return pl.ds(direction * (M // 2), M // 2) if hop == H - 1 else pl.ds(0, M)

    def arrived_gather(w, direction, hop):
        source = (y + 2 * NY - hop - 1) % NY if direction == 0 else (y + hop + 1) % NY
        block = xb.at[w, source, c, span(direction, hop)]
        pltpu.make_async_copy(block, block, ag_rs.at[w, direction, hop]).wait()

    def sibling_copy(w, source, index):
        block = xb.at[w, source, c]
        return pltpu.make_async_remote_copy(
            block, block, sib_ss.at[w, index], sib_rs.at[w, index],
            device_id=(e, sib_t), device_id_type=MESH,
        )

    def sibling_arrived(w, source, index):
        block = xb.at[w, source, 1 - c]
        pltpu.make_async_copy(block, block, sib_rs.at[w, index]).wait()

    def multiply(w, source, fresh):
        rows = jnp.concatenate([xb[w, source, 0], xb[w, source, 1]], axis=1)
        depth = pl.ds(pl.multiple_of(source * 2 * LANES, 2 * LANES), 2 * LANES)
        for k, weight in enumerate((wg, wu)):
            product = dot(rows, weight[depth, :])
            if fresh:
                acc[w, k] = product
            else:
                acc[w, k] += product

    for w in range(2):
        block = xb.at[w, y, c]
        pltpu.make_async_copy(block, block, dsp_rs.at[w]).wait()
        gather_copy(w, 0, 0).start()
        gather_copy(w, 1, 0).start()
        sibling_copy(w, y, 0).start()

    def turn(hop):
        return (y + NY - hop) % NY, (y + hop) % NY

    def multiply_hop(hop):
        for w in range(2):
            for k, source in enumerate(turn(hop) if hop else (y,)):
                index = 2 * hop - 1 + k if hop else 0
                sibling_arrived(w, source, index)
                multiply(w, source, hop == 0)

    far = (y + H) % NY

    def pair_copy(v, half):
        return pltpu.make_async_remote_copy(
            part.at[v, half, 1 - c], pair.at[v, half], sp_ss.at[v, half], sp_rs.at[v, half],
            device_id=(e, sib_t), device_id_type=MESH,
        )

    def down(v, hidden):
        hp[...] = dot(perm[...], hidden).astype(BF)
        for half in range(2):
            product = dot(hp[...], wd[:, half * HALF : (half + 1) * HALF]).astype(BF)
            part[v, half] = product.reshape(2, NY, K, HALF)
            pair_copy(v, half).start()

    def sum_copy(v, direction, step, half):
        return pltpu.make_async_remote_copy(
            sums.at[v, direction, step, half], came.at[v, direction, step, half],
            rs_ss.at[v, direction, step, half], rs_rs.at[v, direction, step, half],
            device_id=(e, right_t if direction == 0 else left_t), device_id_type=MESH,
        )

    def travels(direction, step, half):
        return step > 0 or half == direction

    def pair_sum(v, half, to):
        return part[v, half, c, to].astype(F32) + pair[v, half, to].astype(F32)

    def reduce_step(v, step):
        for half in range(2):
            if step == 0:
                pair_copy(v, half).wait_recv()
            for direction in range(2):
                if not travels(direction, step, half):
                    continue
                to = (y + H - step) % NY if direction == 0 else (y + NY - H + step) % NY
                value = pair_sum(v, half, to)
                if step > 0 and travels(direction, step - 1, half):
                    sum_copy(v, direction, step - 1, half).wait_recv()
                    value = value + came[v, direction, step - 1, half].astype(F32)
                sums[v, direction, step, half] = value.astype(BF)
                sum_copy(v, direction, step, half).start()

    def send_back(v):
        for half in range(2):
            value = pair_sum(v, half, y)
            for direction in range(2):
                if travels(direction, H - 1, half):
                    sum_copy(v, direction, H - 1, half).wait_recv()
                    value = value + came[v, direction, H - 1, half].astype(F32)
            for j in range(HALF // LANES):
                place = half * (HALF // LANES) + j
                stk[pl.ds(place, K, stride=T), :] = value[:, j * LANES : (j + 1) * LANES]
        back[v] = stk[...].astype(BF)
        for place in range(K):
            rows = pl.ds(place * T, T)
            w, slot = (v, K + place) if v < 2 else (place // G, (v - 2) * G + place % G)
            if slot == 0:
                ret_recv[w, own_rows] = back[v, rows, :]
            else:
                pltpu.make_async_remote_copy(
                    back.at[v, rows], ret_recv.at[w, own_rows], ret_ss.at[v], ret_rs.at[w],
                    device_id=(source_of(slot), t), device_id_type=MESH,
                ).start()

    def mate_copy(g):
        return pltpu.make_async_remote_copy(
            xn.at[g, c], xn.at[g, c], mate_ss.at[g], mate_rs.at[g],
            device_id=(e, sib_t), device_id_type=MESH,
        )

    def near_arrived(g):
        others = GT - T if g == 0 else GT
        if others:
            rows = xn.at[g, c, pl.ds(0, others)]
            pltpu.make_async_copy(rows, rows, near_rs.at[g]).wait()
        mate_copy(g).start()

    def near_wave(g):
        other = xn.at[g, 1 - c]
        pltpu.make_async_copy(other, other, mate_rs.at[g]).wait()
        rows = xn[g].reshape(M, D)
        hidden = jax.nn.silu(dot(rows, wg[...])) * dot(rows, wu[...])
        down(2 + g, hidden.astype(BF))

    def far_wave(w):
        sibling_arrived(w, far, NY - 1)
        multiply(w, far, False)
        down(w, (jax.nn.silu(acc[w, 0]) * acc[w, 1]).astype(BF))

    def gather_hop(hop):
        rights, lefts = turn(hop)
        for w in range(2):
            arrived_gather(w, 0, hop - 1)
            arrived_gather(w, 1, hop - 1)
            if hop == H:
                sibling_copy(w, far, NY - 1).start()
                continue
            gather_copy(w, 0, hop).start()
            gather_copy(w, 1, hop).start()
            sibling_copy(w, rights, 2 * hop - 1).start()
            sibling_copy(w, lefts, 2 * hop).start()

    def at(s):
        return pl.ds(pl.multiple_of(s * 8, 8), 8)

    def summing(s, held):
        hf, pf, hb, pb = held
        a, b = af[at(s), :], bf[at(s), :]
        a2, b2 = ab[at(NS - 1 - s), :], bb[at(NS - 1 - s), :]
        return a * hf + b, a * pf, a2 * hb + b2, a2 * pb

    zero, one = jnp.zeros((8, LANES), F32), jnp.ones((8, LANES), F32)
    hf, pf, hb, pb = lax.fori_loop(0, NS, summing, (zero, one, zero, one), unroll=8)
    for k, value in enumerate((pf, hf, pb, hb)):
        seg[k] = value

    def segment(k, g):
        return seg[k, g : g + 1, :]

    ones = jnp.ones((1, LANES), F32)
    fa, fb, ba, bb_ = ones, ones * 0.0, ones, ones * 0.0
    for g in range(8):
        fa, fb = segment(0, g) * fa, segment(0, g) * fb + segment(1, g)
        ba, bb_ = segment(2, 7 - g) * ba, segment(2, 7 - g) * bb_ + segment(3, 7 - g)
    ahead = jnp.concatenate([fa, fb], axis=0)
    behind = jnp.concatenate([ba, bb_], axis=0)
    carry_send[0] = ahead
    carry_send[1] = behind
    carry_recv[e] = ahead

    def send_carry(i, _):
        peer = (e + i) % E
        pltpu.make_async_remote_copy(
            carry_send.at[(peer < e).astype(I32)], carry_recv.at[e], carry_ss, carry_rs,
            device_id=(peer, t), device_id_type=MESH,
        ).start()
        return 0

    lax.fori_loop(1, E, send_carry, 0)

    near_arrived(0)
    loads[2].wait()
    loads[3].wait()
    loads[5].wait()
    for hop in range(1, H + 1):
        gather_hop(hop)
        if hop > 1 or H == 1:
            reduce_step(2, max(0, hop - 2))
        multiply_hop(hop - 1)
        if hop == 1:
            near_wave(0)
        if hop == max(1, H - 1):
            near_arrived(1)
    far_wave(0)
    far_wave(1)
    for step in range(max(1, H - 1), H):
        reduce_step(2, step)
    reduce_step(0, 0)
    reduce_step(1, 0)
    near_wave(1)
    for step in range(1, H):
        reduce_step(0, step)
        reduce_step(1, step)
        if step == 1:
            send_back(2)
        reduce_step(3, step - 1)
    send_back(0)
    send_back(1)
    reduce_step(3, H - 1)
    send_back(3)

    shares_t = scores_t[...] / (scores_t[0:1, :] + scores_t[1:2, :])
    share_of = jnp.where(first_t, shares_t[0:1, :], 0.0) + jnp.where(second_t, shares_t[1:2, :], 0.0)
    own_row = t * EXIT + (iota((T * EXIT, R), 0) & (EXIT - 1))
    rows_out = one_hot(own_row == iota((T * EXIT, R), 1))
    columns_out = one_hot(iota((E, N), 0) == shr(iota((E, N), 1), lT))
    same_tile = shr(iota((T * EXIT, N), 0), 4) == (iota((T * EXIT, N), 1) & (T - 1))
    for w in range(2):
        weight = jnp.where(rank_t == float(w), share_of, 0.0)
        high = weight.astype(BF)
        low = (weight - high.astype(F32)).astype(BF)
        for piece, table in ((high, c_hi), (low, c_lo)):
            picked = lax.dot_general(rows_out, piece, (((1,), (1,)), ((), ())), preferred_element_type=F32)
            wide = dot(picked.astype(BF), columns_out)
            table[w] = jnp.where(same_tile, wide, 0.0).astype(BF)

    pltpu.make_async_copy(
        carry_recv.at[pl.ds(0, E - 1)], carry_recv.at[pl.ds(0, E - 1)], carry_rs
    ).wait()

    def fold(i, held):
        f, b = held
        one_way = carry_recv[i]
        j = E - 1 - i
        other = carry_recv[j]
        f = jnp.where(i < e, one_way[0:1] * f + one_way[1:2], f)
        b = jnp.where(j > e, other[0:1] * b + other[1:2], b)
        return f, b

    f, b = lax.fori_loop(0, E, fold, (ones * 0.0, ones * 0.0))
    f_rows, b_rows = [f], [b]
    for g in range(7):
        f_rows.append(segment(0, g) * f_rows[-1] + segment(1, g))
        b_rows.insert(0, segment(2, 7 - g) * b_rows[0] + segment(3, 7 - g))
    f_in, b_in = jnp.concatenate(f_rows, axis=0), jnp.concatenate(b_rows, axis=0)

    def states(s, held):
        hf, hb = held
        r = NS - 1 - s
        hf = af[at(s), :] * hf + bf[at(s), :]
        hb = ab[at(r), :] * hb + bb[at(r), :]
        bf[at(s), :] = hf
        bb[at(r), :] = hb
        return hf, hb

    lax.fori_loop(0, NS, states, (f_in, b_in), unroll=8)

    def natural(s, _):
        ynat[pl.ds(s, 8, stride=NS), :] = bf[at(s), :] + bb[at(s), :]
        return 0

    lax.fori_loop(0, NS, natural, 0, unroll=8)
    loads[4].wait()

    def finish(i, _):
        rows = pl.ds(pl.multiple_of(i * CH, CH), CH)
        rec_out[rows, :] = (ynat[rows, :] * jax.nn.gelu(gatev[rows, :].astype(F32))).astype(BF)
        return 0

    lax.fori_loop(0, S // CH, finish, 0)

    arrivals = pl.ds(0, (E - 1) * T)
    out = jnp.zeros((T * EXIT, LANES), F32)
    for w in range(2):
        block = ret_recv.at[w, arrivals]
        pltpu.make_async_copy(block, block, ret_rs.at[w]).wait()
        out = out + dot(c_hi[w], ret_recv[w]) + dot(c_lo[w], ret_recv[w])
    for j in range(T):
        exp_out[:, j * LANES : (j + 1) * LANES] = out[j * EXIT : (j + 1) * EXIT, :].astype(BF)

    tail.wait_send()
    head.wait_send()
    sent = [(carry_recv.at[pl.ds(0, E - 1)], carry_ss), (near_send.at[1], near_ss.at[1])]
    sent += [(dsp.at[w], dsp_ss.at[w]) for w in range(2)]
    sent += [(back.at[v], ret_ss.at[v]) for v in (0, 1, 3)]
    if G > 1:
        sent += [(near_send.at[0, pl.ds(0, GT - T)], near_ss.at[0])]
        sent += [(back.at[2, pl.ds(0, M - 2 * T)], ret_ss.at[2])]
    for g in range(2):
        mate_copy(g).wait_send()
    for block, sem in sent:
        pltpu.make_async_copy(block, block, sem).wait()
    for w in range(2):
        for hop in range(H):
            for direction in range(2):
                gather_copy(w, direction, hop).wait_send()
        for index in range(NY):
            sibling_copy(w, y, index).wait_send()
    for v in range(4):
        for half in range(2):
            pair_copy(v, half).wait_send()
            for direction in range(2):
                for step in range(H):
                    if travels(direction, step, half):
                        sum_copy(v, direction, step, half).wait_send()


def local(
    E, T, x_path, gate_path, conv_taps, decay_gate_w, input_gate_w, decay_rate, decay_shift,
    expert_in, norm_gain, routes, route_scores, gate_weight, up_weight, down_weight,
):
    S = x_path.shape[0]
    R, D = expert_in.shape
    F = gate_weight.shape[2]
    NY, H, K, HALF = T // 2, T // 4, E // 2, D // 2
    N, M = E * T, K * T
    anywhere = pl.BlockSpec(memory_space=pl.ANY)
    vmem = pl.BlockSpec(memory_space=pltpu.VMEM)
    dma = pltpu.SemaphoreType.DMA
    rows = pltpu.VMEM((S, LANES), F32)
    scratch = [
        pltpu.VMEM((S, LANES), BF),
        pltpu.VMEM((S, LANES), BF),
        pltpu.VMEM((R, D), BF),
        pltpu.VMEM((D, F), BF),
        pltpu.VMEM((D, F), BF),
        pltpu.VMEM((F, D), BF),
        pltpu.VMEM((2, EXIT, LANES), BF),
        pltpu.VMEM((S + 2 * EXIT, LANES), F32),
        rows,
        rows,
        rows,
        rows,
        rows,
        rows,
        rows,
        pltpu.VMEM((4, 8, LANES), F32),
        pltpu.VMEM((2, 2, LANES), F32),
        pltpu.VMEM((E, 2, LANES), F32),
        pltpu.VMEM((2, E, R), F32),
        pltpu.VMEM((2, M, R), BF),
        pltpu.VMEM((M, R), BF),
        pltpu.VMEM((R, D), BF),
        pltpu.VMEM((2, M, LANES), BF),
        pltpu.VMEM((2, M // 2, D), BF),
        pltpu.VMEM((2, NY, 2, M, LANES), BF),
        pltpu.VMEM((2, 2, M // 2, D), BF),
        pltpu.VMEM((2, 2, M, F), F32),
        pltpu.VMEM((M, M), BF),
        pltpu.VMEM((M, F), BF),
        pltpu.VMEM((4, 2, 2, NY, K, HALF), BF),
        pltpu.VMEM((4, 2, NY, K, HALF), BF),
        pltpu.VMEM((4, 2, H, 2, K, HALF), BF),
        pltpu.VMEM((4, 2, H, 2, K, HALF), BF),
        pltpu.VMEM((M, LANES), F32),
        pltpu.VMEM((4, M, LANES), BF),
        pltpu.VMEM((2, N, LANES), BF),
        pltpu.VMEM((2, T * EXIT, N), BF),
        pltpu.VMEM((2, T * EXIT, N), BF),
        dma((6,)),
        dma((2,)),
        dma((2,)),
        dma,
        dma,
        dma((2,)),
        dma((2,)),
        dma((2,)),
        dma((2,)),
        dma((2,)),
        dma((2,)),
        dma((2, 2, H)),
        dma((2, 2, H)),
        dma((2, NY)),
        dma((2, NY)),
        dma((4, 2)),
        dma((4, 2)),
        dma((4, 2, H, 2)),
        dma((4, 2, H, 2)),
        dma((4,)),
        dma((2,)),
    ]
    return pl.pallas_call(
        functools.partial(layer, E, T),
        out_shape=(
            jax.ShapeDtypeStruct((S, LANES), BF),
            jax.ShapeDtypeStruct((EXIT, D), BF),
        ),
        in_specs=[anywhere] * 6 + [vmem] * 8,
        out_specs=(vmem, vmem),
        scratch_shapes=scratch,
        compiler_params=pltpu.CompilerParams(
            collective_id=0, has_side_effects=True, vmem_limit_bytes=60 * 1024 * 1024
        ),
        name="layer",
    )(
        x_path,
        gate_path,
        expert_in,
        gate_weight.reshape(D, F),
        up_weight.reshape(D, F),
        down_weight.reshape(F, D),
        conv_taps,
        decay_gate_w,
        input_gate_w,
        decay_rate,
        decay_shift.reshape(8, S // 8),
        norm_gain.reshape(D // LANES, LANES),
        routes.T,
        route_scores.T,
    )


def solution(mesh):
    in_specs = (
        P("ep", "tp"),
        P("ep", "tp"),
        P(None, "tp"),
        P(None, "tp", None, None),
        P(None, "tp", None, None),
        P(None, "tp"),
        P("ep", "tp"),
        P("ep", None),
        P(),
        P("ep", None),
        P("ep", None),
        P("ep", None, "tp"),
        P("ep", None, "tp"),
        P("ep", "tp", None),
    )
    out_specs = (P("ep", "tp"), P(("ep", "tp"), None))
    step = functools.partial(local, mesh.shape["ep"], mesh.shape["tp"])
    return jax.shard_map(step, mesh=mesh, in_specs=in_specs, out_specs=out_specs, check_vma=False)
```

```python
import functools

import jax
import jax.numpy as jnp
from jax import lax
from jax.experimental import pallas as pl
from jax.experimental.pallas import tpu as pltpu
from jax.sharding import PartitionSpec as P

BF = jnp.bfloat16
F32 = jnp.float32
I32 = jnp.int32
MESH = pl.DeviceIdType.MESH
EPSILON = 1e-06
LANES = 128
EXIT = 16


def log2(n):
    return n.bit_length() - 1


def iota(shape, dim):
    return lax.broadcasted_iota(I32, shape, dim)


def shr(x, n):
    return lax.shift_right_logical(x, jnp.full(x.shape, n, I32))


def dot(a, b):
    return jnp.dot(a, b, preferred_element_type=F32)


def one_hot(mask):
    return jnp.where(mask, 1.0, 0.0).astype(BF)


def one_minus_square(log_a, a):
    z = 2.0 * log_a
    series = 1.0 + z * (1 / 2 + z * (1 / 6 + z * (1 / 24 + z * (1 / 120 + z * (1 / 720)))))
    return jnp.where(z > -0.25, -z * series, 1.0 - a * a)


def plane(E):
    X = 4 if E >= 32 else min(2, E)
    Z = E // X
    near = (
        [(0, 0), (0, 1), (0, 3), (1, 0), (7, 0), (1, 1), (7, 3), (0, 2)]
        + [(1, 3), (7, 1), (1, 2), (7, 2), (2, 0), (6, 0), (2, 1), (6, 3)]
        if E == 32
        else [(i // X, i % X) for i in range(E // 2)]
    )
    rest = [(z, x) for z in range(Z) for x in range(X) if (z, x) not in near]
    rest.sort(key=lambda p: -(min(p[0], Z - p[0]) + min(p[1], X - p[1])))
    return X, Z, near + rest


def layer(
    E,
    T,
    x_hbm,
    gate_hbm,
    ein_hbm,
    wg_hbm,
    wu_hbm,
    wd_hbm,
    taps_hbm,
    dgw_hbm,
    igw_hbm,
    rate_hbm,
    shift_hbm,
    gain_hbm,
    routes_hbm,
    scores_hbm,
    rec_hbm,
    exp_hbm,
    xraw,
    gatev,
    ein,
    wg,
    wu,
    wd,
    taps,
    dgw,
    igw,
    rate,
    shift,
    gain,
    routes_t,
    scores_t,
    rec_out,
    exp_out,
    halo,
    xpad,
    sh,
    cperm,
    af,
    bf,
    ab,
    bb,
    ynat,
    seg,
    carry_send,
    carry_recv,
    named_as,
    far_select,
    near_select,
    normed,
    dsp,
    near_send,
    xb,
    xn,
    acc,
    perm,
    hp,
    part,
    pair,
    sums,
    came,
    stk,
    back,
    ret_recv,
    c_hi,
    c_lo,
    load_sem,
    store_sem,
    halo_ss,
    halo_rs,
    carry_ss,
    carry_rs,
    dsp_ss,
    dsp_rs,
    near_ss,
    near_rs,
    mate_ss,
    mate_rs,
    ag_ss,
    ag_rs,
    sib_ss,
    sib_rs,
    sp_ss,
    sp_rs,
    rs_ss,
    rs_rs,
    ret_ss,
    ret_rs,
):
    NY, H, K, G = T // 2, T // 4, E // 2, E // 4
    S = xraw.shape[0]
    NS = S // 8
    R, D = ein.shape
    F = wg.shape[1]
    HALF = D // 2
    N, M, GT = E * T, K * T, G * T
    lT, lNY = log2(T), log2(NY)
    X, Z, slots = plane(E)

    e = lax.axis_index("ep")
    t = lax.axis_index("tp")
    y = t // 2
    c = t % 2
    sib_t = y * 2 + (1 - c)
    right_t = ((y + 1) % NY) * 2 + c
    left_t = ((y + NY - 1) % NY) * 2 + c
    ep_next = (e + 1) % E
    ep_prev = (e + E - 1) % E
    ez, ex = e // X, e % X

    def source_of(slot):
        dz, dx = slots[slot]
        return ((ez + dz) % Z) * X + (ex + dx) % X

    def target_of(slot):
        dz, dx = slots[slot]
        return ((ez + Z - dz) % Z) * X + (ex + X - dx) % X

    barrier = pltpu.get_barrier_semaphore()

    greeted = list(range(K)) + list(range(E - 1, K - 1, -1))

    pairs = (
        (routes_hbm, routes_t),
        (ein_hbm, ein),
        (gain_hbm, gain),
        (x_hbm, xraw),
        (taps_hbm, taps),
        (shift_hbm, shift),
        (rate_hbm, rate),
        (dgw_hbm, dgw),
        (igw_hbm, igw),
        (scores_hbm, scores_t),
        (wg_hbm, wg),
        (wu_hbm, wu),
        (wd_hbm, wd),
        (gate_hbm, gatev),
    )
    loads = [pltpu.make_async_copy(src, dst, load_sem.at[i]) for i, (src, dst) in enumerate(pairs)]
    stores = [
        pltpu.make_async_copy(rec_out, rec_hbm, store_sem.at[0]),
        pltpu.make_async_copy(exp_out, exp_hbm, store_sem.at[1]),
    ]
    for load in loads[:4]:
        load.start()
    for slot in range(E - 1, 0, -1):
        pl.semaphore_signal(barrier, inc=1, device_id=(target_of(greeted[slot]), t), device_id_type=MESH)
    for peer in (sib_t, right_t, left_t):
        pl.semaphore_signal(barrier, inc=1, device_id=(e, peer), device_id_type=MESH)
    for load in loads[4:]:
        load.start()

    loads[0].wait()
    ids = iota((E, R), 0)
    first_t = routes_t[0:1, :] == ids
    second_t = routes_t[1:2, :] == ids
    named_t = one_hot(first_t | second_t)
    rr, rc = iota((R, R), 0), iota((R, R), 1)
    earlier_t = one_hot((shr(rr, 4) == shr(rc, 4)) & (rr < rc))
    rank_t = dot(named_t, earlier_t)
    for w in range(2):
        named_as[w] = jnp.where(rank_t == float(w), named_t.astype(F32), 0.0)
    in_block = iota((T, R), 0) == shr(iota((T, R), 1), 4)

    def selector(w, slot):
        named = named_as[w, pl.ds(target_of(slot), 1), :]
        return jnp.where(in_block, jnp.broadcast_to(named, (T, R)), 0.0).astype(BF)

    for w in range(2):
        for j in range(K):
            far_select[w, j * T : (j + 1) * T, :] = selector(w, K + j)
    loads[1].wait()
    loads[2].wait()
    total = jnp.zeros((R, LANES), F32)
    for j in range(D // LANES):
        tile = ein[:, j * LANES : (j + 1) * LANES].astype(F32)
        total = total + tile * tile
    scale = lax.rsqrt(jnp.sum(total, axis=1, keepdims=True) * (1.0 / D) + EPSILON)

    def normed_tile(j):
        columns = pl.ds(pl.multiple_of(j * LANES, LANES), LANES)
        return (ein[:, columns].astype(F32) * scale * gain[pl.ds(j, 1), :]).astype(BF)

    own_normed = normed_tile(t)
    for w in range(2):
        dsp[w] = dot(far_select[w], own_normed).astype(BF)

    loads[3].wait()
    pl.semaphore_wait(barrier, E + 2)

    tail = pltpu.make_async_remote_copy(
        xraw.at[pl.ds(S - EXIT, EXIT)], halo.at[0], halo_ss.at[0], halo_rs.at[0],
        device_id=(ep_next, t), device_id_type=MESH,
    )
    head = pltpu.make_async_remote_copy(
        xraw.at[pl.ds(0, EXIT)], halo.at[1], halo_ss.at[1], halo_rs.at[1],
        device_id=(ep_prev, t), device_id_type=MESH,
    )
    tail.start()
    head.start()

    own_rows = pl.ds(pl.multiple_of(e * T, T), T)
    for w in range(2):
        for j in range(K):
            rows = pl.ds(j * T, T)
            pltpu.make_async_remote_copy(
                dsp.at[w, rows], xb.at[w, y, c, rows], dsp_ss.at[w], dsp_rs.at[w],
                device_id=(target_of(K + j), t), device_id_type=MESH,
            ).start()

    for j in range(D // LANES):
        normed[:, j * LANES : (j + 1) * LANES] = normed_tile(j)
    for k in range(K):
        near_select[k * T : (k + 1) * T, :] = selector(c, k)
    near_send[...] = dot(near_select[...], normed[...]).astype(BF).reshape(2, GT, D)

    def send_near(g):
        for k in range(G):
            rows = pl.ds(k * T, T)
            if g + k == 0:
                xn[g, c, rows, :] = near_send[g, rows, :]
                continue
            pltpu.make_async_remote_copy(
                near_send.at[g, rows], xn.at[g, c, rows], near_ss.at[g], near_rs.at[g],
                device_id=(target_of(g * G + k), t), device_id_type=MESH,
            ).start()

    send_near(0)

    n0, n1 = iota((M, M), 0), iota((M, M), 1)
    perm_block = (shr(n0, log2(K)) & (NY - 1)) * 2 + shr(n0, log2(K) + lNY)
    perm[...] = one_hot((shr(n1, lT) == (n0 & (K - 1))) & ((n1 & (T - 1)) == perm_block))

    for load in loads[4:9]:
        load.wait()
    xpad[pl.ds(EXIT, S), :] = xraw[...].astype(F32)
    for s in range(NS):
        sh[pl.ds(s * 8, 8), :] = jnp.broadcast_to(shift[:, s : s + 1], (8, LANES))
    tail.wait_recv()
    head.wait_recv()
    xpad[pl.ds(0, EXIT), :] = jnp.where(e > 0, halo[0].astype(F32), 0.0)
    xpad[pl.ds(EXIT + S, EXIT), :] = jnp.where(e < E - 1, halo[1].astype(F32), 0.0)

    def strided(s):
        return xpad[pl.ds(EXIT + s, 8, stride=NS), :]

    tap = [taps[k : k + 1, :] for k in range(4)]

    def conv(s, held):
        v0, v1, v2 = held
        v3 = strided(s + 1)
        value = v0 * tap[0] + v1 * tap[1] + v2 * tap[2] + v3 * tap[3]
        cperm[pl.ds(pl.multiple_of(s * 8, 8), 8), :] = value.astype(BF).astype(F32)
        return v1, v2, v3

    lax.fori_loop(0, NS, conv, (strided(-2), strided(-1), strided(0)), unroll=8)

    def gather_copy(w, direction, hop):
        source = (y + NY - hop) % NY if direction == 0 else (y + hop) % NY
        block = xb.at[w, source, c, span(direction, hop)]
        return pltpu.make_async_remote_copy(
            block, block, ag_ss.at[w, direction, hop], ag_rs.at[w, direction, hop],
            device_id=(e, right_t if direction == 0 else left_t), device_id_type=MESH,
        )

    def span(direction, hop):
        return pl.ds(direction * (M // 2), M // 2) if hop == H - 1 else pl.ds(0, M)

    def arrived_gather(w, direction, hop):
        source = (y + 2 * NY - hop - 1) % NY if direction == 0 else (y + hop + 1) % NY
        block = xb.at[w, source, c, span(direction, hop)]
        pltpu.make_async_copy(block, block, ag_rs.at[w, direction, hop]).wait()

    def sibling_copy(w, source, index):
        block = xb.at[w, source, c]
        return pltpu.make_async_remote_copy(
            block, block, sib_ss.at[w, index], sib_rs.at[w, index],
            device_id=(e, sib_t), device_id_type=MESH,
        )

    def sibling_arrived(w, source, index):
        block = xb.at[w, source, 1 - c]
        pltpu.make_async_copy(block, block, sib_rs.at[w, index]).wait()

    def multiply(w, source, fresh):
        rows = jnp.concatenate([xb[w, source, 0], xb[w, source, 1]], axis=1)
        depth = pl.ds(pl.multiple_of(source * 2 * LANES, 2 * LANES), 2 * LANES)
        for k, weight in enumerate((wg, wu)):
            product = dot(rows, weight[depth, :])
            if fresh:
                acc[w, k] = product
            else:
                acc[w, k] += product

    send_near(1)
    for w in range(2):
        block = xb.at[w, y, c]
        pltpu.make_async_copy(block, block, dsp_rs.at[w]).wait()
        gather_copy(w, 0, 0).start()
        gather_copy(w, 1, 0).start()
        sibling_copy(w, y, 0).start()

    def turn(hop):
        return (y + NY - hop) % NY, (y + hop) % NY

    def multiply_hop(hop, w):
        for k, source in enumerate(turn(hop) if hop else (y,)):
            index = 2 * hop - 1 + k if hop else 0
            sibling_arrived(w, source, index)
            multiply(w, source, hop == 0)

    far = (y + H) % NY

    def pair_copy(v, half):
        return pltpu.make_async_remote_copy(
            part.at[v, half, 1 - c], pair.at[v, half], sp_ss.at[v, half], sp_rs.at[v, half],
            device_id=(e, sib_t), device_id_type=MESH,
        )

    def down(v, hidden):
        hp[...] = dot(perm[...], hidden).astype(BF)
        for half in range(2):
            product = dot(hp[...], wd[:, half * HALF : (half + 1) * HALF]).astype(BF)
            part[v, half] = product.reshape(2, NY, K, HALF)
            pair_copy(v, half).start()

    def sum_copy(v, direction, step, half):
        return pltpu.make_async_remote_copy(
            sums.at[v, direction, step, half], came.at[v, direction, step, half],
            rs_ss.at[v, direction, step, half], rs_rs.at[v, direction, step, half],
            device_id=(e, right_t if direction == 0 else left_t), device_id_type=MESH,
        )

    def travels(direction, step, half):
        return step > 0 or half == direction

    def pair_sum(v, half, to):
        return part[v, half, c, to].astype(F32) + pair[v, half, to].astype(F32)

    def reduce_step(v, step):
        for half in range(2):
            if step == 0:
                pair_copy(v, half).wait_recv()
            for direction in range(2):
                if not travels(direction, step, half):
                    continue
                to = (y + H - step) % NY if direction == 0 else (y + NY - H + step) % NY
                value = pair_sum(v, half, to)
                if step > 0 and travels(direction, step - 1, half):
                    sum_copy(v, direction, step - 1, half).wait_recv()
                    value = value + came[v, direction, step - 1, half].astype(F32)
                sums[v, direction, step, half] = value.astype(BF)
                sum_copy(v, direction, step, half).start()

    def send_back(v):
        for half in range(2):
            value = pair_sum(v, half, y)
            for direction in range(2):
                if travels(direction, H - 1, half):
                    sum_copy(v, direction, H - 1, half).wait_recv()
                    value = value + came[v, direction, H - 1, half].astype(F32)
            for j in range(HALF // LANES):
                place = half * (HALF // LANES) + j
                stk[pl.ds(place, K, stride=T), :] = value[:, j * LANES : (j + 1) * LANES]
        back[v] = stk[...].astype(BF)
        for place in range(K):
            rows = pl.ds(place * T, T)
            w, slot = (v, K + place) if v < 2 else (place // G, (v - 2) * G + place % G)
            if slot == 0:
                ret_recv[w, own_rows] = back[v, rows, :]
            else:
                pltpu.make_async_remote_copy(
                    back.at[v, rows], ret_recv.at[w, own_rows], ret_ss.at[v], ret_rs.at[w],
                    device_id=(source_of(slot), t), device_id_type=MESH,
                ).start()

    def mate_copy(g):
        return pltpu.make_async_remote_copy(
            xn.at[g, c], xn.at[g, c], mate_ss.at[g], mate_rs.at[g],
            device_id=(e, sib_t), device_id_type=MESH,
        )

    def near_arrived(g):
        others = GT - T if g == 0 else GT
        if others:
            rows = xn.at[g, c, pl.ds(0, others)]
            pltpu.make_async_copy(rows, rows, near_rs.at[g]).wait()
        mate_copy(g).start()

    def near_wave(g):
        other = xn.at[g, 1 - c]
        pltpu.make_async_copy(other, other, mate_rs.at[g]).wait()
        rows = xn[g].reshape(M, D)
        hidden = jax.nn.silu(dot(rows, wg[...])) * dot(rows, wu[...])
        down(2 + g, hidden.astype(BF))

    def far_wave(w):
        sibling_arrived(w, far, NY - 1)
        multiply(w, far, False)
        down(w, (jax.nn.silu(acc[w, 0]) * acc[w, 1]).astype(BF))

    def gather_hop(hop, w):
        rights, lefts = turn(hop)
        arrived_gather(w, 0, hop - 1)
        if hop < H:
            gather_copy(w, 0, hop).start()
        arrived_gather(w, 1, hop - 1)
        if hop < H:
            gather_copy(w, 1, hop).start()
            sibling_copy(w, rights, 2 * hop - 1).start()
            sibling_copy(w, lefts, 2 * hop).start()
        else:
            sibling_copy(w, far, NY - 1).start()

    CH = min(128, S)

    def gates(i, _):
        rows = pl.ds(pl.multiple_of(i * CH, CH), CH)
        value = cperm[rows, :]
        value_b = value.astype(BF)
        shift_here = sh[rows, :]
        for d, (a_ref, b_ref) in enumerate(((af, bf), (ab, bb))):
            decay_gate = jax.nn.sigmoid(dot(value_b, dgw[d, 0]))
            input_gate = jax.nn.sigmoid(dot(value_b, igw[d, 0]))
            log_decay = -8.0 * decay_gate * rate[d : d + 1, :] + shift_here
            decay = jnp.exp(log_decay)
            rest = one_minus_square(log_decay, decay)
            root = rest * lax.rsqrt(jnp.maximum(rest, 1e-37))
            a_ref[rows, :] = decay
            b_ref[rows, :] = root * input_gate * value
        return 0

    lax.fori_loop(0, S // CH, gates, 0)

    def at(s):
        return pl.ds(pl.multiple_of(s * 8, 8), 8)

    def summing(s, held):
        hf, pf, hb, pb = held
        a, b = af[at(s), :], bf[at(s), :]
        a2, b2 = ab[at(NS - 1 - s), :], bb[at(NS - 1 - s), :]
        return a * hf + b, a * pf, a2 * hb + b2, a2 * pb

    zero, one = jnp.zeros((8, LANES), F32), jnp.ones((8, LANES), F32)
    hf, pf, hb, pb = lax.fori_loop(0, NS, summing, (zero, one, zero, one), unroll=8)
    for k, value in enumerate((pf, hf, pb, hb)):
        seg[k] = value

    def segment(k, g):
        return seg[k, g : g + 1, :]

    ones = jnp.ones((1, LANES), F32)
    fa, fb, ba, bb_ = ones, ones * 0.0, ones, ones * 0.0
    for g in range(8):
        fa, fb = segment(0, g) * fa, segment(0, g) * fb + segment(1, g)
        ba, bb_ = segment(2, 7 - g) * ba, segment(2, 7 - g) * bb_ + segment(3, 7 - g)
    ahead = jnp.concatenate([fa, fb], axis=0)
    behind = jnp.concatenate([ba, bb_], axis=0)
    carry_send[0] = ahead
    carry_send[1] = behind
    carry_recv[e] = ahead

    def send_carry(i, _):
        peer = (e + i) % E
        pltpu.make_async_remote_copy(
            carry_send.at[(peer < e).astype(I32)], carry_recv.at[e], carry_ss, carry_rs,
            device_id=(peer, t), device_id_type=MESH,
        ).start()
        return 0

    lax.fori_loop(1, E, send_carry, 0)

    def second_pass():
        pltpu.make_async_copy(
            carry_recv.at[pl.ds(0, E - 1)], carry_recv.at[pl.ds(0, E - 1)], carry_rs
        ).wait()

        def fold(i, held):
            f, b = held
            one_way = carry_recv[i]
            j = E - 1 - i
            other = carry_recv[j]
            f = jnp.where(i < e, one_way[0:1] * f + one_way[1:2], f)
            b = jnp.where(j > e, other[0:1] * b + other[1:2], b)
            return f, b

        f, b = lax.fori_loop(0, E, fold, (ones * 0.0, ones * 0.0))
        f_rows, b_rows = [f], [b]
        for g in range(7):
            f_rows.append(segment(0, g) * f_rows[-1] + segment(1, g))
            b_rows.insert(0, segment(2, 7 - g) * b_rows[0] + segment(3, 7 - g))
        f_in, b_in = jnp.concatenate(f_rows, axis=0), jnp.concatenate(b_rows, axis=0)

        def states(s, held):
            hf, hb = held
            r = NS - 1 - s
            hf = af[at(s), :] * hf + bf[at(s), :]
            hb = ab[at(r), :] * hb + bb[at(r), :]
            bf[at(s), :] = hf
            bb[at(r), :] = hb
            return hf, hb

        lax.fori_loop(0, NS, states, (f_in, b_in), unroll=8)

        def natural(s, _):
            ynat[pl.ds(s, 8, stride=NS), :] = bf[at(s), :] + bb[at(s), :]
            return 0

        lax.fori_loop(0, NS, natural, 0, unroll=8)
        loads[13].wait()

        def finish(i, _):
            rows = pl.ds(pl.multiple_of(i * CH, CH), CH)
            rec_out[rows, :] = (ynat[rows, :] * jax.nn.gelu(gatev[rows, :].astype(F32))).astype(BF)
            return 0

        lax.fori_loop(0, S // CH, finish, 0)
        stores[0].start()

    near_arrived(0)
    for load in loads[10:13]:
        load.wait()
    for hop in range(1, H):
        for w in range(2):
            gather_hop(hop, w)
        if hop == H - 1:
            near_arrived(1)
        if hop > 1:
            reduce_step(2, hop - 2)
        for w in range(2):
            multiply_hop(hop - 1, w)
        if hop == 1:
            near_wave(0)
    near_wave(1)
    for w in range(2):
        gather_hop(H, w)
        multiply_hop(H - 1, w)
    reduce_step(2, H - 2)
    reduce_step(3, 0)
    far_wave(0)
    far_wave(1)
    reduce_step(0, 0)
    reduce_step(2, H - 1)
    reduce_step(1, 0)
    reduce_step(3, 1)
    for step in range(1, H):
        reduce_step(0, step)
        reduce_step(1, step)
        if step == 1:
            send_back(2)
        if step + 1 < H:
            reduce_step(3, step + 1)
    send_back(3)
    send_back(0)
    send_back(1)
    loads[9].wait()
    shares_t = scores_t[...] / (scores_t[0:1, :] + scores_t[1:2, :])
    share_of = jnp.where(first_t, shares_t[0:1, :], 0.0) + jnp.where(second_t, shares_t[1:2, :], 0.0)
    own_row = t * EXIT + (iota((T * EXIT, R), 0) & (EXIT - 1))
    rows_out = one_hot(own_row == iota((T * EXIT, R), 1))
    columns_out = one_hot(iota((E, N), 0) == shr(iota((E, N), 1), lT))
    same_tile = shr(iota((T * EXIT, N), 0), 4) == (iota((T * EXIT, N), 1) & (T - 1))
    for w in range(2):
        weight = jnp.where(rank_t == float(w), share_of, 0.0)
        high = weight.astype(BF)
        low = (weight - high.astype(F32)).astype(BF)
        for piece, table in ((high, c_hi), (low, c_lo)):
            picked = lax.dot_general(rows_out, piece, (((1,), (1,)), ((), ())), preferred_element_type=F32)
            wide = dot(picked.astype(BF), columns_out)
            table[w] = jnp.where(same_tile, wide, 0.0).astype(BF)

    second_pass()
    arrivals = pl.ds(0, (E - 1) * T)
    out = jnp.zeros((T * EXIT, LANES), F32)
    for w in range(2):
        block = ret_recv.at[w, arrivals]
        pltpu.make_async_copy(block, block, ret_rs.at[w]).wait()
        out = out + dot(c_hi[w], ret_recv[w]) + dot(c_lo[w], ret_recv[w])
    for j in range(T):
        exp_out[:, j * LANES : (j + 1) * LANES] = out[j * EXIT : (j + 1) * EXIT, :].astype(BF)
    stores[1].start()

    tail.wait_send()
    head.wait_send()
    sent = [(carry_recv.at[pl.ds(0, E - 1)], carry_ss), (near_send.at[1], near_ss.at[1])]
    sent += [(dsp.at[w], dsp_ss.at[w]) for w in range(2)]
    sent += [(back.at[v], ret_ss.at[v]) for v in (0, 1, 3)]
    if G > 1:
        sent += [(near_send.at[0, pl.ds(0, GT - T)], near_ss.at[0])]
        sent += [(back.at[2, pl.ds(0, M - 2 * T)], ret_ss.at[2])]
    for g in range(2):
        mate_copy(g).wait_send()
    for block, sem in sent:
        pltpu.make_async_copy(block, block, sem).wait()
    for w in range(2):
        for hop in range(H):
            for direction in range(2):
                gather_copy(w, direction, hop).wait_send()
        for index in range(NY):
            sibling_copy(w, y, index).wait_send()
    for v in range(4):
        for half in range(2):
            pair_copy(v, half).wait_send()
            for direction in range(2):
                for step in range(H):
                    if travels(direction, step, half):
                        sum_copy(v, direction, step, half).wait_send()
    for store in stores:
        store.wait()


def local(
    E, T, x_path, gate_path, conv_taps, decay_gate_w, input_gate_w, decay_rate, decay_shift,
    expert_in, norm_gain, routes, route_scores, gate_weight, up_weight, down_weight,
):
    S = x_path.shape[0]
    R, D = expert_in.shape
    F = gate_weight.shape[2]
    NY, H, K, HALF = T // 2, T // 4, E // 2, D // 2
    N, M = E * T, K * T
    hbm = pl.BlockSpec(memory_space=pltpu.HBM)
    dma = pltpu.SemaphoreType.DMA
    rows = pltpu.VMEM((S, LANES), F32)
    scratch = [
        pltpu.VMEM((S, LANES), BF),
        pltpu.VMEM((S, LANES), BF),
        pltpu.VMEM((R, D), BF),
        pltpu.VMEM((D, F), BF),
        pltpu.VMEM((D, F), BF),
        pltpu.VMEM((F, D), BF),
        pltpu.VMEM((4, LANES), F32),
        pltpu.VMEM((2, 1, LANES, LANES), BF),
        pltpu.VMEM((2, 1, LANES, LANES), BF),
        pltpu.VMEM((2, LANES), F32),
        pltpu.VMEM((8, S // 8), F32),
        pltpu.VMEM((D // LANES, LANES), F32),
        pltpu.VMEM((2, R), I32),
        pltpu.VMEM((2, R), F32),
        pltpu.VMEM((S, LANES), BF),
        pltpu.VMEM((EXIT, D), BF),
        pltpu.VMEM((2, EXIT, LANES), BF),
        pltpu.VMEM((S + 2 * EXIT, LANES), F32),
        rows,
        rows,
        rows,
        rows,
        rows,
        rows,
        rows,
        pltpu.VMEM((4, 8, LANES), F32),
        pltpu.VMEM((2, 2, LANES), F32),
        pltpu.VMEM((E, 2, LANES), F32),
        pltpu.VMEM((2, E, R), F32),
        pltpu.VMEM((2, M, R), BF),
        pltpu.VMEM((M, R), BF),
        pltpu.VMEM((R, D), BF),
        pltpu.VMEM((2, M, LANES), BF),
        pltpu.VMEM((2, M // 2, D), BF),
        pltpu.VMEM((2, NY, 2, M, LANES), BF),
        pltpu.VMEM((2, 2, M // 2, D), BF),
        pltpu.VMEM((2, 2, M, F), F32),
        pltpu.VMEM((M, M), BF),
        pltpu.VMEM((M, F), BF),
        pltpu.VMEM((4, 2, 2, NY, K, HALF), BF),
        pltpu.VMEM((4, 2, NY, K, HALF), BF),
        pltpu.VMEM((4, 2, H, 2, K, HALF), BF),
        pltpu.VMEM((4, 2, H, 2, K, HALF), BF),
        pltpu.VMEM((M, LANES), F32),
        pltpu.VMEM((4, M, LANES), BF),
        pltpu.VMEM((2, N, LANES), BF),
        pltpu.VMEM((2, T * EXIT, N), BF),
        pltpu.VMEM((2, T * EXIT, N), BF),
        dma((14,)),
        dma((2,)),
        dma((2,)),
        dma((2,)),
        dma,
        dma,
        dma((2,)),
        dma((2,)),
        dma((2,)),
        dma((2,)),
        dma((2,)),
        dma((2,)),
        dma((2, 2, H)),
        dma((2, 2, H)),
        dma((2, NY)),
        dma((2, NY)),
        dma((4, 2)),
        dma((4, 2)),
        dma((4, 2, H, 2)),
        dma((4, 2, H, 2)),
        dma((4,)),
        dma((2,)),
    ]
    return pl.pallas_call(
        functools.partial(layer, E, T),
        out_shape=(
            jax.ShapeDtypeStruct((S, LANES), BF),
            jax.ShapeDtypeStruct((EXIT, D), BF),
        ),
        in_specs=[hbm] * 14,
        out_specs=(hbm, hbm),
        scratch_shapes=scratch,
        compiler_params=pltpu.CompilerParams(
            collective_id=0, has_side_effects=True, vmem_limit_bytes=60 * 1024 * 1024
        ),
        name="layer",
    )(
        x_path,
        gate_path,
        expert_in,
        gate_weight.reshape(D, F),
        up_weight.reshape(D, F),
        down_weight.reshape(F, D),
        conv_taps,
        decay_gate_w,
        input_gate_w,
        decay_rate,
        decay_shift.reshape(8, S // 8),
        norm_gain.reshape(D // LANES, LANES),
        routes.T,
        route_scores.T,
    )


def solution(mesh):
    in_specs = (
        P("ep", "tp"),
        P("ep", "tp"),
        P(None, "tp"),
        P(None, "tp", None, None),
        P(None, "tp", None, None),
        P(None, "tp"),
        P("ep", "tp"),
        P("ep", None),
        P(),
        P("ep", None),
        P("ep", None),
        P("ep", None, "tp"),
        P("ep", None, "tp"),
        P("ep", "tp", None),
    )
    out_specs = (P("ep", "tp"), P(("ep", "tp"), None))
    step = functools.partial(local, mesh.shape["ep"], mesh.shape["tp"])
    return jax.shard_map(step, mesh=mesh, in_specs=in_specs, out_specs=out_specs, check_vma=False)
```

```python
import functools

import jax
import jax.numpy as jnp
from jax import lax
from jax.experimental import pallas as pl
from jax.experimental.pallas import tpu as pltpu
from jax.sharding import PartitionSpec as P

BF = jnp.bfloat16
F32 = jnp.float32
I32 = jnp.int32
MESH = pl.DeviceIdType.MESH
EPSILON = 1e-06
LANES = 128
EXIT = 16


def log2(n):
    return n.bit_length() - 1


def iota(shape, dim):
    return lax.broadcasted_iota(I32, shape, dim)


def shr(x, n):
    return lax.shift_right_logical(x, jnp.full(x.shape, n, I32))


def dot(a, b):
    return jnp.dot(a, b, preferred_element_type=F32)


def one_hot(mask):
    return jnp.where(mask, 1.0, 0.0).astype(BF)


def one_minus_square(log_a, a):
    z = 2.0 * log_a
    series = 1.0 + z * (1 / 2 + z * (1 / 6 + z * (1 / 24 + z * (1 / 120 + z * (1 / 720)))))
    return jnp.where(z > -0.25, -z * series, 1.0 - a * a)


def plane(E):
    X = 4 if E >= 32 else min(2, E)
    Z = E // X
    near = (
        [(0, 0), (0, 1), (0, 3), (1, 0), (7, 0), (1, 1), (7, 3), (0, 2)]
        + [(1, 3), (7, 1), (1, 2), (7, 2), (2, 0), (6, 0), (2, 1), (6, 3)]
        if E == 32
        else [(i // X, i % X) for i in range(E // 2)]
    )
    rest = [(z, x) for z in range(Z) for x in range(X) if (z, x) not in near]
    rest.sort(key=lambda p: -(min(p[0], Z - p[0]) + min(p[1], X - p[1])))
    return X, Z, near + rest


def layer(
    E,
    T,
    x_hbm,
    gate_hbm,
    ein_hbm,
    wg_hbm,
    wu_hbm,
    wd_hbm,
    taps_hbm,
    dgw_hbm,
    igw_hbm,
    rate_hbm,
    shift_hbm,
    gain_hbm,
    routes_hbm,
    scores_hbm,
    rec_hbm,
    exp_hbm,
    xraw,
    gatev,
    ein,
    wg,
    wu,
    wd,
    taps,
    dgw,
    igw,
    rate,
    shift,
    gain,
    routes_t,
    scores_t,
    rec_out,
    exp_out,
    halo,
    xpad,
    sh,
    cperm,
    af,
    bf,
    ab,
    bb,
    ynat,
    seg,
    carry_send,
    carry_recv,
    named_as,
    far_select,
    near_select,
    normed,
    dsp,
    near_send,
    xb,
    xn,
    acc,
    perm,
    hp,
    part,
    pair,
    sums,
    came,
    stk,
    back,
    ret_recv,
    c_hi,
    c_lo,
    load_sem,
    store_sem,
    halo_ss,
    halo_rs,
    carry_ss,
    carry_rs,
    dsp_ss,
    dsp_rs,
    near_ss,
    near_rs,
    mate_ss,
    mate_rs,
    ag_ss,
    ag_rs,
    sib_ss,
    sib_rs,
    sp_ss,
    sp_rs,
    rs_ss,
    rs_rs,
    ret_ss,
    ret_rs,
):
    NY, H, K, G = T // 2, T // 4, E // 2, E // 4
    S = xraw.shape[0]
    NS = S // 8
    R, D = ein.shape
    F = wg.shape[1]
    HALF = D // 2
    N, M, GT = E * T, K * T, G * T
    lT, lNY = log2(T), log2(NY)
    X, Z, slots = plane(E)

    e = lax.axis_index("ep")
    t = lax.axis_index("tp")
    y = t // 2
    c = t % 2
    sib_t = y * 2 + (1 - c)
    right_t = ((y + 1) % NY) * 2 + c
    left_t = ((y + NY - 1) % NY) * 2 + c
    ep_next = (e + 1) % E
    ep_prev = (e + E - 1) % E
    ez, ex = e // X, e % X

    def source_of(slot):
        dz, dx = slots[slot]
        return ((ez + dz) % Z) * X + (ex + dx) % X

    def target_of(slot):
        dz, dx = slots[slot]
        return ((ez + Z - dz) % Z) * X + (ex + X - dx) % X

    barrier = pltpu.get_barrier_semaphore()

    greeted = list(range(K)) + list(range(E - 1, K - 1, -1))

    pairs = (
        (routes_hbm, routes_t),
        (ein_hbm, ein),
        (gain_hbm, gain),
        (x_hbm, xraw),
        (taps_hbm, taps),
        (shift_hbm, shift),
        (rate_hbm, rate),
        (dgw_hbm, dgw),
        (igw_hbm, igw),
        (scores_hbm, scores_t),
        (wg_hbm, wg),
        (wu_hbm, wu),
        (wd_hbm, wd),
        (gate_hbm, gatev),
    )
    loads = [pltpu.make_async_copy(src, dst, load_sem.at[i]) for i, (src, dst) in enumerate(pairs)]
    stores = [
        pltpu.make_async_copy(rec_out, rec_hbm, store_sem.at[0]),
        pltpu.make_async_copy(exp_out, exp_hbm, store_sem.at[1]),
    ]
    for load in loads[:4]:
        load.start()
    for slot in range(E - 1, 0, -1):
        pl.semaphore_signal(barrier, inc=1, device_id=(target_of(greeted[slot]), t), device_id_type=MESH)
    for peer in (sib_t, right_t, left_t):
        pl.semaphore_signal(barrier, inc=1, device_id=(e, peer), device_id_type=MESH)
    for load in loads[4:]:
        load.start()

    loads[0].wait()
    ids = iota((E, R), 0)
    first_t = routes_t[0:1, :] == ids
    second_t = routes_t[1:2, :] == ids
    named_t = one_hot(first_t | second_t)
    rr, rc = iota((R, R), 0), iota((R, R), 1)
    earlier_t = one_hot((shr(rr, 4) == shr(rc, 4)) & (rr < rc))
    rank_t = dot(named_t, earlier_t)
    for w in range(2):
        named_as[w] = jnp.where(rank_t == float(w), named_t.astype(F32), 0.0)
    in_block = iota((T, R), 0) == shr(iota((T, R), 1), 4)

    def selector(w, slot):
        named = named_as[w, pl.ds(target_of(slot), 1), :]
        return jnp.where(in_block, jnp.broadcast_to(named, (T, R)), 0.0).astype(BF)

    for w in range(2):
        for j in range(K):
            far_select[w, j * T : (j + 1) * T, :] = selector(w, K + j)
    loads[1].wait()
    loads[2].wait()
    total = jnp.zeros((R, LANES), F32)
    for j in range(D // LANES):
        tile = ein[:, j * LANES : (j + 1) * LANES].astype(F32)
        total = total + tile * tile
    scale = lax.rsqrt(jnp.sum(total, axis=1, keepdims=True) * (1.0 / D) + EPSILON)

    def normed_tile(j):
        columns = pl.ds(pl.multiple_of(j * LANES, LANES), LANES)
        return (ein[:, columns].astype(F32) * scale * gain[pl.ds(j, 1), :]).astype(BF)

    own_normed = normed_tile(t)
    for w in range(2):
        dsp[w] = dot(far_select[w], own_normed).astype(BF)

    loads[3].wait()
    pl.semaphore_wait(barrier, E + 2)

    tail = pltpu.make_async_remote_copy(
        xraw.at[pl.ds(S - EXIT, EXIT)], halo.at[0], halo_ss.at[0], halo_rs.at[0],
        device_id=(ep_next, t), device_id_type=MESH,
    )
    head = pltpu.make_async_remote_copy(
        xraw.at[pl.ds(0, EXIT)], halo.at[1], halo_ss.at[1], halo_rs.at[1],
        device_id=(ep_prev, t), device_id_type=MESH,
    )
    tail.start()
    head.start()

    own_rows = pl.ds(pl.multiple_of(e * T, T), T)
    for w in range(2):
        for j in range(K):
            rows = pl.ds(j * T, T)
            pltpu.make_async_remote_copy(
                dsp.at[w, rows], xb.at[w, y, c, rows], dsp_ss.at[w], dsp_rs.at[w],
                device_id=(target_of(K + j), t), device_id_type=MESH,
            ).start()

    for j in range(D // LANES):
        normed[:, j * LANES : (j + 1) * LANES] = normed_tile(j)
    for k in range(K):
        near_select[k * T : (k + 1) * T, :] = selector(c, k)
    near_send[...] = dot(near_select[...], normed[...]).astype(BF).reshape(2, GT, D)

    def send_near(g):
        for k in range(G):
            rows = pl.ds(k * T, T)
            if g + k == 0:
                xn[g, c, rows, :] = near_send[g, rows, :]
                continue
            pltpu.make_async_remote_copy(
                near_send.at[g, rows], xn.at[g, c, rows], near_ss.at[g], near_rs.at[g, k],
                device_id=(target_of(g * G + k), t), device_id_type=MESH,
            ).start()

    send_near(0)

    n0, n1 = iota((M, M), 0), iota((M, M), 1)
    perm_block = (shr(n0, log2(K)) & (NY - 1)) * 2 + shr(n0, log2(K) + lNY)
    perm[...] = one_hot((shr(n1, lT) == (n0 & (K - 1))) & ((n1 & (T - 1)) == perm_block))

    for load in loads[4:9]:
        load.wait()
    xpad[pl.ds(EXIT, S), :] = xraw[...].astype(F32)
    for s in range(NS):
        sh[pl.ds(s * 8, 8), :] = jnp.broadcast_to(shift[:, s : s + 1], (8, LANES))
    tail.wait_recv()
    head.wait_recv()
    xpad[pl.ds(0, EXIT), :] = jnp.where(e > 0, halo[0].astype(F32), 0.0)
    xpad[pl.ds(EXIT + S, EXIT), :] = jnp.where(e < E - 1, halo[1].astype(F32), 0.0)

    def strided(s):
        return xpad[pl.ds(EXIT + s, 8, stride=NS), :]

    tap = [taps[k : k + 1, :] for k in range(4)]

    def conv(s, held):
        v0, v1, v2 = held
        v3 = strided(s + 1)
        value = v0 * tap[0] + v1 * tap[1] + v2 * tap[2] + v3 * tap[3]
        cperm[pl.ds(pl.multiple_of(s * 8, 8), 8), :] = value.astype(BF).astype(F32)
        return v1, v2, v3

    lax.fori_loop(0, NS, conv, (strided(-2), strided(-1), strided(0)), unroll=8)

    CH = min(128, S)

    def gates(i, _):
        rows = pl.ds(pl.multiple_of(i * CH, CH), CH)
        value = cperm[rows, :]
        value_b = value.astype(BF)
        shift_here = sh[rows, :]
        for d, (a_ref, b_ref) in enumerate(((af, bf), (ab, bb))):
            decay_gate = jax.nn.sigmoid(dot(value_b, dgw[d, 0]))
            input_gate = jax.nn.sigmoid(dot(value_b, igw[d, 0]))
            log_decay = -8.0 * decay_gate * rate[d : d + 1, :] + shift_here
            decay = jnp.exp(log_decay)
            rest = one_minus_square(log_decay, decay)
            root = rest * lax.rsqrt(jnp.maximum(rest, 1e-37))
            a_ref[rows, :] = decay
            b_ref[rows, :] = root * input_gate * value
        return 0

    lax.fori_loop(0, S // CH, gates, 0)

    def gather_copy(w, direction, hop):
        source = (y + NY - hop) % NY if direction == 0 else (y + hop) % NY
        block = xb.at[w, source, c, span(direction, hop)]
        return pltpu.make_async_remote_copy(
            block, block, ag_ss.at[w, direction, hop], ag_rs.at[w, direction, hop],
            device_id=(e, right_t if direction == 0 else left_t), device_id_type=MESH,
        )

    def span(direction, hop):
        return pl.ds(direction * (M // 2), M // 2) if hop == H - 1 else pl.ds(0, M)

    def arrived_gather(w, direction, hop):
        source = (y + 2 * NY - hop - 1) % NY if direction == 0 else (y + hop + 1) % NY
        block = xb.at[w, source, c, span(direction, hop)]
        pltpu.make_async_copy(block, block, ag_rs.at[w, direction, hop]).wait()

    def sibling_copy(w, source, index):
        block = xb.at[w, source, c]
        return pltpu.make_async_remote_copy(
            block, block, sib_ss.at[w, index], sib_rs.at[w, index],
            device_id=(e, sib_t), device_id_type=MESH,
        )

    def sibling_arrived(w, source, index):
        block = xb.at[w, source, 1 - c]
        pltpu.make_async_copy(block, block, sib_rs.at[w, index]).wait()

    def multiply(w, source, fresh):
        rows = jnp.concatenate([xb[w, source, 0], xb[w, source, 1]], axis=1)
        depth = pl.ds(pl.multiple_of(source * 2 * LANES, 2 * LANES), 2 * LANES)
        for k, weight in enumerate((wg, wu)):
            product = dot(rows, weight[depth, :])
            if fresh:
                acc[w, k] = product
            else:
                acc[w, k] += product

    send_near(1)
    for w in range(2):
        block = xb.at[w, y, c]
        pltpu.make_async_copy(block, block, dsp_rs.at[w]).wait()
        gather_copy(w, 0, 0).start()
        gather_copy(w, 1, 0).start()
        sibling_copy(w, y, 0).start()

    def turn(hop):
        return (y + NY - hop) % NY, (y + hop) % NY

    def multiply_hop(hop, w):
        for k, source in enumerate(turn(hop) if hop else (y,)):
            index = 2 * hop - 1 + k if hop else 0
            sibling_arrived(w, source, index)
            multiply(w, source, hop == 0)

    far = (y + H) % NY

    def pair_copy(v, half):
        return pltpu.make_async_remote_copy(
            part.at[v, half, 1 - c], pair.at[v, half], sp_ss.at[v, half], sp_rs.at[v, half],
            device_id=(e, sib_t), device_id_type=MESH,
        )

    def down(v, hidden):
        hp[...] = dot(perm[...], hidden).astype(BF)
        for half in range(2):
            product = dot(hp[...], wd[:, half * HALF : (half + 1) * HALF]).astype(BF)
            part[v, half] = product.reshape(2, NY, K, HALF)
            pair_copy(v, half).start()

    def sum_copy(v, direction, step, half):
        return pltpu.make_async_remote_copy(
            sums.at[v, direction, step, half], came.at[v, direction, step, half],
            rs_ss.at[v, direction, step, half], rs_rs.at[v, direction, step, half],
            device_id=(e, right_t if direction == 0 else left_t), device_id_type=MESH,
        )

    def travels(direction, step, half):
        return step > 0 or half == direction

    def pair_sum(v, half, to):
        return part[v, half, c, to].astype(F32) + pair[v, half, to].astype(F32)

    def reduce_step(v, step):
        for half in range(2):
            if step == 0:
                pair_copy(v, half).wait_recv()
            for direction in range(2):
                if not travels(direction, step, half):
                    continue
                to = (y + H - step) % NY if direction == 0 else (y + NY - H + step) % NY
                value = pair_sum(v, half, to)
                if step > 0 and travels(direction, step - 1, half):
                    sum_copy(v, direction, step - 1, half).wait_recv()
                    value = value + came[v, direction, step - 1, half].astype(F32)
                sums[v, direction, step, half] = value.astype(BF)
                sum_copy(v, direction, step, half).start()

    def send_back(v):
        for half in range(2):
            value = pair_sum(v, half, y)
            for direction in range(2):
                if travels(direction, H - 1, half):
                    sum_copy(v, direction, H - 1, half).wait_recv()
                    value = value + came[v, direction, H - 1, half].astype(F32)
            for j in range(HALF // LANES):
                place = half * (HALF // LANES) + j
                stk[pl.ds(place, K, stride=T), :] = value[:, j * LANES : (j + 1) * LANES]
        back[v] = stk[...].astype(BF)
        for place in range(K):
            rows = pl.ds(place * T, T)
            w, slot = (v, K + place) if v < 2 else (place // G, (v - 2) * G + place % G)
            if slot == 0:
                ret_recv[w, own_rows] = back[v, rows, :]
            else:
                pltpu.make_async_remote_copy(
                    back.at[v, rows], ret_recv.at[w, own_rows], ret_ss.at[v], ret_rs.at[w],
                    device_id=(source_of(slot), t), device_id_type=MESH,
                ).start()

    def near_arrived(g, first, last):
        for k in range(first, last):
            rows = xn.at[g, c, pl.ds(k * T, T)]
            if g + k:
                pltpu.make_async_copy(rows, rows, near_rs.at[g, k]).wait()
            pltpu.make_async_remote_copy(
                rows, rows, mate_ss.at[g], mate_rs.at[g], device_id=(e, sib_t), device_id_type=MESH
            ).start()

    def near_wave(g):
        other = xn.at[g, 1 - c]
        pltpu.make_async_copy(other, other, mate_rs.at[g]).wait()
        rows = xn[g].reshape(M, D)
        hidden = jax.nn.silu(dot(rows, wg[...])) * dot(rows, wu[...])
        down(2 + g, hidden.astype(BF))

    def far_wave(w):
        sibling_arrived(w, far, NY - 1)
        multiply(w, far, False)
        down(w, (jax.nn.silu(acc[w, 0]) * acc[w, 1]).astype(BF))

    def gather_hop(hop, w):
        rights, lefts = turn(hop)
        arrived_gather(w, 0, hop - 1)
        if hop < H:
            gather_copy(w, 0, hop).start()
        arrived_gather(w, 1, hop - 1)
        if hop < H:
            gather_copy(w, 1, hop).start()
            sibling_copy(w, rights, 2 * hop - 1).start()
            sibling_copy(w, lefts, 2 * hop).start()
        else:
            sibling_copy(w, far, NY - 1).start()

    def at(s):
        return pl.ds(pl.multiple_of(s * 8, 8), 8)

    def summing(s, held):
        hf, pf, hb, pb = held
        a, b = af[at(s), :], bf[at(s), :]
        a2, b2 = ab[at(NS - 1 - s), :], bb[at(NS - 1 - s), :]
        return a * hf + b, a * pf, a2 * hb + b2, a2 * pb

    zero, one = jnp.zeros((8, LANES), F32), jnp.ones((8, LANES), F32)
    hf, pf, hb, pb = lax.fori_loop(0, NS, summing, (zero, one, zero, one), unroll=8)
    for k, value in enumerate((pf, hf, pb, hb)):
        seg[k] = value

    def segment(k, g):
        return seg[k, g : g + 1, :]

    ones = jnp.ones((1, LANES), F32)
    fa, fb, ba, bb_ = ones, ones * 0.0, ones, ones * 0.0
    for g in range(8):
        fa, fb = segment(0, g) * fa, segment(0, g) * fb + segment(1, g)
        ba, bb_ = segment(2, 7 - g) * ba, segment(2, 7 - g) * bb_ + segment(3, 7 - g)
    ahead = jnp.concatenate([fa, fb], axis=0)
    behind = jnp.concatenate([ba, bb_], axis=0)
    carry_send[0] = ahead
    carry_send[1] = behind
    carry_recv[e] = ahead

    def send_carry(i, _):
        peer = (e + i) % E
        pltpu.make_async_remote_copy(
            carry_send.at[(peer < e).astype(I32)], carry_recv.at[e], carry_ss, carry_rs,
            device_id=(peer, t), device_id_type=MESH,
        ).start()
        return 0

    lax.fori_loop(1, E, send_carry, 0)

    def second_pass():
        pltpu.make_async_copy(
            carry_recv.at[pl.ds(0, E - 1)], carry_recv.at[pl.ds(0, E - 1)], carry_rs
        ).wait()

        def fold(i, held):
            f, b = held
            one_way = carry_recv[i]
            j = E - 1 - i
            other = carry_recv[j]
            f = jnp.where(i < e, one_way[0:1] * f + one_way[1:2], f)
            b = jnp.where(j > e, other[0:1] * b + other[1:2], b)
            return f, b

        f, b = lax.fori_loop(0, E, fold, (ones * 0.0, ones * 0.0))
        f_rows, b_rows = [f], [b]
        for g in range(7):
            f_rows.append(segment(0, g) * f_rows[-1] + segment(1, g))
            b_rows.insert(0, segment(2, 7 - g) * b_rows[0] + segment(3, 7 - g))
        f_in, b_in = jnp.concatenate(f_rows, axis=0), jnp.concatenate(b_rows, axis=0)

        def states(s, held):
            hf, hb = held
            r = NS - 1 - s
            hf = af[at(s), :] * hf + bf[at(s), :]
            hb = ab[at(r), :] * hb + bb[at(r), :]
            bf[at(s), :] = hf
            bb[at(r), :] = hb
            return hf, hb

        lax.fori_loop(0, NS, states, (f_in, b_in), unroll=8)

        def natural(s, _):
            ynat[pl.ds(s, 8, stride=NS), :] = bf[at(s), :] + bb[at(s), :]
            return 0

        lax.fori_loop(0, NS, natural, 0, unroll=8)
        loads[13].wait()

        def finish(i, _):
            rows = pl.ds(pl.multiple_of(i * CH, CH), CH)
            rec_out[rows, :] = (ynat[rows, :] * jax.nn.gelu(gatev[rows, :].astype(F32))).astype(BF)
            return 0

        lax.fori_loop(0, S // CH, finish, 0)
        stores[0].start()

    near_arrived(0, 0, G)
    for load in loads[10:13]:
        load.wait()
    for hop in range(1, H):
        for w in range(2):
            gather_hop(hop, w)
        if hop == H - 2:
            near_arrived(1, 0, G // 2)
        if hop == H - 1:
            near_arrived(1, G // 2 if H > 2 else 0, G)
        if hop > 1:
            reduce_step(2, hop - 2)
        for w in range(2):
            multiply_hop(hop - 1, w)
        if hop == 1:
            near_wave(0)
    near_wave(1)
    for w in range(2):
        gather_hop(H, w)
        multiply_hop(H - 1, w)
    reduce_step(2, H - 2)
    reduce_step(3, 0)
    far_wave(0)
    far_wave(1)
    reduce_step(0, 0)
    reduce_step(2, H - 1)
    reduce_step(1, 0)
    reduce_step(3, 1)
    for step in range(1, H):
        reduce_step(0, step)
        reduce_step(1, step)
        if step == 1:
            send_back(2)
        if step + 1 < H:
            reduce_step(3, step + 1)
    send_back(3)
    send_back(0)
    send_back(1)
    loads[9].wait()
    shares_t = scores_t[...] / (scores_t[0:1, :] + scores_t[1:2, :])
    share_of = jnp.where(first_t, shares_t[0:1, :], 0.0) + jnp.where(second_t, shares_t[1:2, :], 0.0)
    own_row = t * EXIT + (iota((T * EXIT, R), 0) & (EXIT - 1))
    rows_out = one_hot(own_row == iota((T * EXIT, R), 1))
    columns_out = one_hot(iota((E, N), 0) == shr(iota((E, N), 1), lT))
    same_tile = shr(iota((T * EXIT, N), 0), 4) == (iota((T * EXIT, N), 1) & (T - 1))
    for w in range(2):
        weight = jnp.where(rank_t == float(w), share_of, 0.0)
        high = weight.astype(BF)
        low = (weight - high.astype(F32)).astype(BF)
        for piece, table in ((high, c_hi), (low, c_lo)):
            picked = lax.dot_general(rows_out, piece, (((1,), (1,)), ((), ())), preferred_element_type=F32)
            wide = dot(picked.astype(BF), columns_out)
            table[w] = jnp.where(same_tile, wide, 0.0).astype(BF)

    second_pass()
    arrivals = pl.ds(0, (E - 1) * T)
    out = jnp.zeros((T * EXIT, LANES), F32)
    for w in range(2):
        block = ret_recv.at[w, arrivals]
        pltpu.make_async_copy(block, block, ret_rs.at[w]).wait()
        out = out + dot(c_hi[w], ret_recv[w]) + dot(c_lo[w], ret_recv[w])
    for j in range(T):
        exp_out[:, j * LANES : (j + 1) * LANES] = out[j * EXIT : (j + 1) * EXIT, :].astype(BF)
    stores[1].start()

    tail.wait_send()
    head.wait_send()
    sent = [(carry_recv.at[pl.ds(0, E - 1)], carry_ss), (near_send.at[1], near_ss.at[1])]
    sent += [(dsp.at[w], dsp_ss.at[w]) for w in range(2)]
    sent += [(back.at[v], ret_ss.at[v]) for v in (0, 1, 3)]
    if G > 1:
        sent += [(near_send.at[0, pl.ds(0, GT - T)], near_ss.at[0])]
        sent += [(back.at[2, pl.ds(0, M - 2 * T)], ret_ss.at[2])]
    sent += [(xn.at[g, c], mate_ss.at[g]) for g in range(2)]
    for block, sem in sent:
        pltpu.make_async_copy(block, block, sem).wait()
    for w in range(2):
        for hop in range(H):
            for direction in range(2):
                gather_copy(w, direction, hop).wait_send()
        for index in range(NY):
            sibling_copy(w, y, index).wait_send()
    for v in range(4):
        for half in range(2):
            pair_copy(v, half).wait_send()
            for direction in range(2):
                for step in range(H):
                    if travels(direction, step, half):
                        sum_copy(v, direction, step, half).wait_send()
    for store in stores:
        store.wait()


def hand_over(rec_in, exp_in, rec_out, exp_out, rec, exp, in_sem, out_sem):
    loads = [
        pltpu.make_async_copy(rec_in, rec, in_sem.at[0]),
        pltpu.make_async_copy(exp_in, exp, in_sem.at[1]),
    ]
    stores = [
        pltpu.make_async_copy(rec, rec_out, out_sem.at[0]),
        pltpu.make_async_copy(exp, exp_out, out_sem.at[1]),
    ]
    for load in loads:
        load.start()
    for load, store in zip(loads, stores):
        load.wait()
        store.start()
    for store in stores:
        store.wait()


def local(
    E, T, x_path, gate_path, conv_taps, decay_gate_w, input_gate_w, decay_rate, decay_shift,
    expert_in, norm_gain, routes, route_scores, gate_weight, up_weight, down_weight,
):
    S = x_path.shape[0]
    R, D = expert_in.shape
    F = gate_weight.shape[2]
    NY, H, K, G, HALF = T // 2, T // 4, E // 2, E // 4, D // 2
    N, M = E * T, K * T
    hbm = pl.BlockSpec(memory_space=pltpu.HBM)
    dma = pltpu.SemaphoreType.DMA
    rows = pltpu.VMEM((S, LANES), F32)
    scratch = [
        pltpu.VMEM((S, LANES), BF),
        pltpu.VMEM((S, LANES), BF),
        pltpu.VMEM((R, D), BF),
        pltpu.VMEM((D, F), BF),
        pltpu.VMEM((D, F), BF),
        pltpu.VMEM((F, D), BF),
        pltpu.VMEM((4, LANES), F32),
        pltpu.VMEM((2, 1, LANES, LANES), BF),
        pltpu.VMEM((2, 1, LANES, LANES), BF),
        pltpu.VMEM((2, LANES), F32),
        pltpu.VMEM((8, S // 8), F32),
        pltpu.VMEM((D // LANES, LANES), F32),
        pltpu.VMEM((2, R), I32),
        pltpu.VMEM((2, R), F32),
        pltpu.VMEM((S, LANES), BF),
        pltpu.VMEM((EXIT, D), BF),
        pltpu.VMEM((2, EXIT, LANES), BF),
        pltpu.VMEM((S + 2 * EXIT, LANES), F32),
        rows,
        rows,
        rows,
        rows,
        rows,
        rows,
        rows,
        pltpu.VMEM((4, 8, LANES), F32),
        pltpu.VMEM((2, 2, LANES), F32),
        pltpu.VMEM((E, 2, LANES), F32),
        pltpu.VMEM((2, E, R), F32),
        pltpu.VMEM((2, M, R), BF),
        pltpu.VMEM((M, R), BF),
        pltpu.VMEM((R, D), BF),
        pltpu.VMEM((2, M, LANES), BF),
        pltpu.VMEM((2, M // 2, D), BF),
        pltpu.VMEM((2, NY, 2, M, LANES), BF),
        pltpu.VMEM((2, 2, M // 2, D), BF),
        pltpu.VMEM((2, 2, M, F), F32),
        pltpu.VMEM((M, M), BF),
        pltpu.VMEM((M, F), BF),
        pltpu.VMEM((4, 2, 2, NY, K, HALF), BF),
        pltpu.VMEM((4, 2, NY, K, HALF), BF),
        pltpu.VMEM((4, 2, H, 2, K, HALF), BF),
        pltpu.VMEM((4, 2, H, 2, K, HALF), BF),
        pltpu.VMEM((M, LANES), F32),
        pltpu.VMEM((4, M, LANES), BF),
        pltpu.VMEM((2, N, LANES), BF),
        pltpu.VMEM((2, T * EXIT, N), BF),
        pltpu.VMEM((2, T * EXIT, N), BF),
        dma((14,)),
        dma((2,)),
        dma((2,)),
        dma((2,)),
        dma,
        dma,
        dma((2,)),
        dma((2,)),
        dma((2,)),
        dma((2, G)),
        dma((2,)),
        dma((2,)),
        dma((2, 2, H)),
        dma((2, 2, H)),
        dma((2, NY)),
        dma((2, NY)),
        dma((4, 2)),
        dma((4, 2)),
        dma((4, 2, H, 2)),
        dma((4, 2, H, 2)),
        dma((4,)),
        dma((2,)),
    ]
    results = pl.pallas_call(
        functools.partial(layer, E, T),
        out_shape=(
            jax.ShapeDtypeStruct((S, LANES), BF),
            jax.ShapeDtypeStruct((EXIT, D), BF),
        ),
        in_specs=[hbm] * 14,
        out_specs=(hbm, hbm),
        scratch_shapes=scratch,
        compiler_params=pltpu.CompilerParams(
            collective_id=0, has_side_effects=True, vmem_limit_bytes=60 * 1024 * 1024
        ),
        name="layer",
    )(
        x_path,
        gate_path,
        expert_in,
        gate_weight.reshape(D, F),
        up_weight.reshape(D, F),
        down_weight.reshape(F, D),
        conv_taps,
        decay_gate_w,
        input_gate_w,
        decay_rate,
        decay_shift.reshape(8, S // 8),
        norm_gain.reshape(D // LANES, LANES),
        routes.T,
        route_scores.T,
    )
    return pl.pallas_call(
        hand_over,
        out_shape=tuple(jax.ShapeDtypeStruct(r.shape, r.dtype) for r in results),
        in_specs=[hbm] * 2,
        out_specs=(hbm, hbm),
        scratch_shapes=[pltpu.VMEM(r.shape, r.dtype) for r in results] + [dma((2,)), dma((2,))],
        compiler_params=pltpu.CompilerParams(vmem_limit_bytes=60 * 1024 * 1024),
        name="hand_over",
    )(*results)


def solution(mesh):
    in_specs = (
        P("ep", "tp"),
        P("ep", "tp"),
        P(None, "tp"),
        P(None, "tp", None, None),
        P(None, "tp", None, None),
        P(None, "tp"),
        P("ep", "tp"),
        P("ep", None),
        P(),
        P("ep", None),
        P("ep", None),
        P("ep", None, "tp"),
        P("ep", None, "tp"),
        P("ep", "tp", None),
    )
    out_specs = (P("ep", "tp"), P(("ep", "tp"), None))
    step = functools.partial(local, mesh.shape["ep"], mesh.shape["tp"])
    return jax.shard_map(step, mesh=mesh, in_specs=in_specs, out_specs=out_specs, check_vma=False)
```

```python
import functools

import jax
import jax.numpy as jnp
from jax import lax
from jax.experimental import pallas as pl
from jax.experimental.pallas import tpu as pltpu
from jax.sharding import PartitionSpec as P

BF = jnp.bfloat16
F32 = jnp.float32
I32 = jnp.int32
MESH = pl.DeviceIdType.MESH
EPSILON = 1e-06
LANES = 128
EXIT = 16


def log2(n):
    return n.bit_length() - 1


def iota(shape, dim):
    return lax.broadcasted_iota(I32, shape, dim)


def shr(x, n):
    return lax.shift_right_logical(x, jnp.full(x.shape, n, I32))


def dot(a, b):
    return jnp.dot(a, b, preferred_element_type=F32)


def one_hot(mask):
    return jnp.where(mask, 1.0, 0.0).astype(BF)


def one_minus_square(log_a, a):
    z = 2.0 * log_a
    series = 1.0 + z * (1 / 2 + z * (1 / 6 + z * (1 / 24 + z * (1 / 120 + z * (1 / 720)))))
    return jnp.where(z > -0.25, -z * series, 1.0 - a * a)


def plane(E):
    X = 4 if E >= 32 else min(2, E)
    Z = E // X
    near = (
        [(0, 0), (0, 1), (0, 3), (1, 0), (7, 0), (1, 1), (7, 3), (0, 2)]
        + [(1, 3), (7, 1), (1, 2), (7, 2), (2, 0), (6, 0), (2, 1), (6, 3)]
        if E == 32
        else [(i // X, i % X) for i in range(E // 2)]
    )
    rest = [(z, x) for z in range(Z) for x in range(X) if (z, x) not in near]
    rest.sort(key=lambda p: -(min(p[0], Z - p[0]) + min(p[1], X - p[1])))
    return X, Z, near + rest


def layer(
    E,
    T,
    x_hbm,
    gate_hbm,
    ein_hbm,
    wg_hbm,
    wu_hbm,
    wd_hbm,
    taps_hbm,
    dgw_hbm,
    igw_hbm,
    rate_hbm,
    shift_hbm,
    gain_hbm,
    routes_hbm,
    scores_hbm,
    rec_hbm,
    exp_hbm,
    xraw,
    gatev,
    ein,
    wg,
    wu,
    wd,
    taps,
    dgw,
    igw,
    rate,
    shift,
    gain,
    routes_t,
    scores_t,
    rec_out,
    exp_out,
    halo,
    xpad,
    sh,
    cperm,
    af,
    bf,
    ab,
    bb,
    ynat,
    seg,
    carry_send,
    carry_recv,
    named_as,
    far_select,
    near_select,
    normed,
    dsp,
    near_send,
    xb,
    xn,
    acc,
    perm,
    hp,
    part,
    pair,
    sums,
    came,
    stk,
    back,
    ret_recv,
    c_hi,
    c_lo,
    load_sem,
    store_sem,
    halo_ss,
    halo_rs,
    carry_ss,
    carry_rs,
    dsp_ss,
    dsp_rs,
    near_ss,
    near_rs,
    mate_ss,
    mate_rs,
    ag_ss,
    ag_rs,
    sib_ss,
    sib_rs,
    sp_ss,
    sp_rs,
    rs_ss,
    rs_rs,
    ret_ss,
    ret_rs,
):
    NY, H, K, G = T // 2, T // 4, E // 2, E // 4
    S = xraw.shape[0]
    NS = S // 8
    R, D = ein.shape
    F = wg.shape[1]
    HALF = D // 2
    N, M, GT = E * T, K * T, G * T
    lT, lNY = log2(T), log2(NY)
    X, Z, slots = plane(E)

    e = lax.axis_index("ep")
    t = lax.axis_index("tp")
    y = t // 2
    c = t % 2
    sib_t = y * 2 + (1 - c)
    right_t = ((y + 1) % NY) * 2 + c
    left_t = ((y + NY - 1) % NY) * 2 + c
    ep_next = (e + 1) % E
    ep_prev = (e + E - 1) % E
    ez, ex = e // X, e % X

    def source_of(slot):
        dz, dx = slots[slot]
        return ((ez + dz) % Z) * X + (ex + dx) % X

    def target_of(slot):
        dz, dx = slots[slot]
        return ((ez + Z - dz) % Z) * X + (ex + X - dx) % X

    barrier = pltpu.get_barrier_semaphore()

    greeted = list(range(K)) + list(range(E - 1, K - 1, -1))

    pairs = (
        (ein_hbm, ein),
        (routes_hbm, routes_t),
        (gain_hbm, gain),
        (x_hbm, xraw),
        (taps_hbm, taps),
        (shift_hbm, shift),
        (rate_hbm, rate),
        (dgw_hbm, dgw),
        (igw_hbm, igw),
        (scores_hbm, scores_t),
        (wg_hbm, wg),
        (wu_hbm, wu),
        (wd_hbm, wd),
        (gate_hbm, gatev),
    )
    loads = [pltpu.make_async_copy(src, dst, load_sem.at[i]) for i, (src, dst) in enumerate(pairs)]
    stores = [
        pltpu.make_async_copy(rec_out, rec_hbm, store_sem.at[0]),
        pltpu.make_async_copy(exp_out, exp_hbm, store_sem.at[1]),
    ]
    for load in loads[:4]:
        load.start()
    for slot in range(E - 1, 0, -1):
        pl.semaphore_signal(barrier, inc=1, device_id=(target_of(greeted[slot]), t), device_id_type=MESH)
    for peer in (sib_t, right_t, left_t):
        pl.semaphore_signal(barrier, inc=1, device_id=(e, peer), device_id_type=MESH)
    for load in loads[4:]:
        load.start()

    loads[1].wait()
    ids = iota((E, R), 0)
    first_t = routes_t[0:1, :] == ids
    second_t = routes_t[1:2, :] == ids
    named_t = one_hot(first_t | second_t)
    rr, rc = iota((R, R), 0), iota((R, R), 1)
    earlier_t = one_hot((shr(rr, 4) == shr(rc, 4)) & (rr < rc))
    rank_t = dot(named_t, earlier_t)
    for w in range(2):
        named_as[w] = jnp.where(rank_t == float(w), named_t.astype(F32), 0.0)
    in_block = iota((T, R), 0) == shr(iota((T, R), 1), 4)

    def selector(w, slot):
        named = named_as[w, pl.ds(target_of(slot), 1), :]
        return jnp.where(in_block, jnp.broadcast_to(named, (T, R)), 0.0).astype(BF)

    for w in range(2):
        for j in range(K):
            far_select[w, j * T : (j + 1) * T, :] = selector(w, K + j)
    loads[0].wait()
    loads[2].wait()
    total = jnp.zeros((R, LANES), F32)
    for j in range(D // LANES):
        tile = ein[:, j * LANES : (j + 1) * LANES].astype(F32)
        total = total + tile * tile
    scale = lax.rsqrt(jnp.sum(total, axis=1, keepdims=True) * (1.0 / D) + EPSILON)

    def normed_tile(j):
        columns = pl.ds(pl.multiple_of(j * LANES, LANES), LANES)
        return (ein[:, columns].astype(F32) * scale * gain[pl.ds(j, 1), :]).astype(BF)

    own_normed = normed_tile(t)
    for w in range(2):
        dsp[w] = dot(far_select[w], own_normed).astype(BF)

    loads[3].wait()
    pl.semaphore_wait(barrier, E + 2)

    tail = pltpu.make_async_remote_copy(
        xraw.at[pl.ds(S - EXIT, EXIT)], halo.at[0], halo_ss.at[0], halo_rs.at[0],
        device_id=(ep_next, t), device_id_type=MESH,
    )
    head = pltpu.make_async_remote_copy(
        xraw.at[pl.ds(0, EXIT)], halo.at[1], halo_ss.at[1], halo_rs.at[1],
        device_id=(ep_prev, t), device_id_type=MESH,
    )
    tail.start()
    head.start()

    own_rows = pl.ds(pl.multiple_of(e * T, T), T)
    for w in range(2):
        for j in range(K):
            rows = pl.ds(j * T, T)
            pltpu.make_async_remote_copy(
                dsp.at[w, rows], xb.at[w, y, c, rows], dsp_ss.at[w], dsp_rs.at[w],
                device_id=(target_of(K + j), t), device_id_type=MESH,
            ).start()

    for j in range(D // LANES):
        normed[:, j * LANES : (j + 1) * LANES] = normed_tile(j)
    for k in range(K):
        near_select[k * T : (k + 1) * T, :] = selector(c, k)
    near_send[...] = dot(near_select[...], normed[...]).astype(BF).reshape(2, GT, D)

    def send_near(g):
        for k in range(G):
            rows = pl.ds(k * T, T)
            if g + k == 0:
                xn[g, c, rows, :] = near_send[g, rows, :]
                continue
            pltpu.make_async_remote_copy(
                near_send.at[g, rows], xn.at[g, c, rows], near_ss.at[g], near_rs.at[g, k],
                device_id=(target_of(g * G + k), t), device_id_type=MESH,
            ).start()

    send_near(0)

    n0, n1 = iota((M, M), 0), iota((M, M), 1)
    perm_block = (shr(n0, log2(K)) & (NY - 1)) * 2 + shr(n0, log2(K) + lNY)
    perm[...] = one_hot((shr(n1, lT) == (n0 & (K - 1))) & ((n1 & (T - 1)) == perm_block))

    for load in loads[4:9]:
        load.wait()
    xpad[pl.ds(EXIT, S), :] = xraw[...].astype(F32)
    for s in range(NS):
        sh[pl.ds(s * 8, 8), :] = jnp.broadcast_to(shift[:, s : s + 1], (8, LANES))
    tail.wait_recv()
    head.wait_recv()
    xpad[pl.ds(0, EXIT), :] = jnp.where(e > 0, halo[0].astype(F32), 0.0)
    xpad[pl.ds(EXIT + S, EXIT), :] = jnp.where(e < E - 1, halo[1].astype(F32), 0.0)

    def strided(s):
        return xpad[pl.ds(EXIT + s, 8, stride=NS), :]

    tap = [taps[k : k + 1, :] for k in range(4)]

    def conv(s, held):
        v0, v1, v2 = held
        v3 = strided(s + 1)
        value = v0 * tap[0] + v1 * tap[1] + v2 * tap[2] + v3 * tap[3]
        cperm[pl.ds(pl.multiple_of(s * 8, 8), 8), :] = value.astype(BF).astype(F32)
        return v1, v2, v3

    lax.fori_loop(0, NS, conv, (strided(-2), strided(-1), strided(0)), unroll=8)

    CH = min(128, S)

    def gates(i, _):
        rows = pl.ds(pl.multiple_of(i * CH, CH), CH)
        value = cperm[rows, :]
        value_b = value.astype(BF)
        shift_here = sh[rows, :]
        for d, (a_ref, b_ref) in enumerate(((af, bf), (ab, bb))):
            decay_gate = jax.nn.sigmoid(dot(value_b, dgw[d, 0]))
            input_gate = jax.nn.sigmoid(dot(value_b, igw[d, 0]))
            log_decay = -8.0 * decay_gate * rate[d : d + 1, :] + shift_here
            decay = jnp.exp(log_decay)
            rest = one_minus_square(log_decay, decay)
            root = rest * lax.rsqrt(jnp.maximum(rest, 1e-37))
            a_ref[rows, :] = decay
            b_ref[rows, :] = root * input_gate * value
        return 0

    lax.fori_loop(0, S // CH, gates, 0)

    def gather_copy(w, direction, hop):
        source = (y + NY - hop) % NY if direction == 0 else (y + hop) % NY
        block = xb.at[w, source, c, span(direction, hop)]
        return pltpu.make_async_remote_copy(
            block, block, ag_ss.at[w, direction, hop], ag_rs.at[w, direction, hop],
            device_id=(e, right_t if direction == 0 else left_t), device_id_type=MESH,
        )

    def span(direction, hop):
        return pl.ds(direction * (M // 2), M // 2) if hop == H - 1 else pl.ds(0, M)

    def arrived_gather(w, direction, hop):
        source = (y + 2 * NY - hop - 1) % NY if direction == 0 else (y + hop + 1) % NY
        block = xb.at[w, source, c, span(direction, hop)]
        pltpu.make_async_copy(block, block, ag_rs.at[w, direction, hop]).wait()

    def sibling_copy(w, source, index):
        block = xb.at[w, source, c]
        return pltpu.make_async_remote_copy(
            block, block, sib_ss.at[w, index], sib_rs.at[w, index],
            device_id=(e, sib_t), device_id_type=MESH,
        )

    def sibling_arrived(w, source, index):
        block = xb.at[w, source, 1 - c]
        pltpu.make_async_copy(block, block, sib_rs.at[w, index]).wait()

    def multiply(w, source, fresh):
        rows = jnp.concatenate([xb[w, source, 0], xb[w, source, 1]], axis=1)
        depth = pl.ds(pl.multiple_of(source * 2 * LANES, 2 * LANES), 2 * LANES)
        for k, weight in enumerate((wg, wu)):
            product = dot(rows, weight[depth, :])
            if fresh:
                acc[w, k] = product
            else:
                acc[w, k] += product

    send_near(1)
    for w in range(2):
        block = xb.at[w, y, c]
        pltpu.make_async_copy(block, block, dsp_rs.at[w]).wait()
        gather_copy(w, 0, 0).start()
        gather_copy(w, 1, 0).start()
        sibling_copy(w, y, 0).start()

    def turn(hop):
        return (y + NY - hop) % NY, (y + hop) % NY

    def multiply_hop(hop, w):
        for k, source in enumerate(turn(hop) if hop else (y,)):
            index = 2 * hop - 1 + k if hop else 0
            sibling_arrived(w, source, index)
            multiply(w, source, hop == 0)

    far = (y + H) % NY

    def pair_copy(v, half):
        return pltpu.make_async_remote_copy(
            part.at[v, half, 1 - c], pair.at[v, half], sp_ss.at[v, half], sp_rs.at[v, half],
            device_id=(e, sib_t), device_id_type=MESH,
        )

    def down(v, hidden):
        hp[...] = dot(perm[...], hidden).astype(BF)
        for half in range(2):
            product = dot(hp[...], wd[:, half * HALF : (half + 1) * HALF]).astype(BF)
            part[v, half] = product.reshape(2, NY, K, HALF)
            pair_copy(v, half).start()

    def sum_copy(v, direction, step, half):
        return pltpu.make_async_remote_copy(
            sums.at[v, direction, step, half], came.at[v, direction, step, half],
            rs_ss.at[v, direction, step, half], rs_rs.at[v, direction, step, half],
            device_id=(e, right_t if direction == 0 else left_t), device_id_type=MESH,
        )

    def travels(direction, step, half):
        return step > 0 or half == direction

    def pair_sum(v, half, to):
        return part[v, half, c, to].astype(F32) + pair[v, half, to].astype(F32)

    def reduce_step(v, step):
        for half in range(2):
            if step == 0:
                pair_copy(v, half).wait_recv()
            for direction in range(2):
                if not travels(direction, step, half):
                    continue
                to = (y + H - step) % NY if direction == 0 else (y + NY - H + step) % NY
                value = pair_sum(v, half, to)
                if step > 0 and travels(direction, step - 1, half):
                    sum_copy(v, direction, step - 1, half).wait_recv()
                    value = value + came[v, direction, step - 1, half].astype(F32)
                sums[v, direction, step, half] = value.astype(BF)
                sum_copy(v, direction, step, half).start()

    def send_back(v):
        for half in range(2):
            value = pair_sum(v, half, y)
            for direction in range(2):
                if travels(direction, H - 1, half):
                    sum_copy(v, direction, H - 1, half).wait_recv()
                    value = value + came[v, direction, H - 1, half].astype(F32)
            for j in range(HALF // LANES):
                place = half * (HALF // LANES) + j
                stk[pl.ds(place, K, stride=T), :] = value[:, j * LANES : (j + 1) * LANES]
        back[v] = stk[...].astype(BF)
        for place in range(K):
            rows = pl.ds(place * T, T)
            w, slot = (v, K + place) if v < 2 else (place // G, (v - 2) * G + place % G)
            if slot == 0:
                ret_recv[w, own_rows] = back[v, rows, :]
            else:
                pltpu.make_async_remote_copy(
                    back.at[v, rows], ret_recv.at[w, own_rows], ret_ss.at[v], ret_rs.at[w],
                    device_id=(source_of(slot), t), device_id_type=MESH,
                ).start()

    def near_arrived(g, first, last):
        for k in range(first, last):
            rows = xn.at[g, c, pl.ds(k * T, T)]
            if g + k:
                pltpu.make_async_copy(rows, rows, near_rs.at[g, k]).wait()
            pltpu.make_async_remote_copy(
                rows, rows, mate_ss.at[g], mate_rs.at[g], device_id=(e, sib_t), device_id_type=MESH
            ).start()

    def near_wave(g):
        other = xn.at[g, 1 - c]
        pltpu.make_async_copy(other, other, mate_rs.at[g]).wait()
        rows = xn[g].reshape(M, D)
        hidden = jax.nn.silu(dot(rows, wg[...])) * dot(rows, wu[...])
        down(2 + g, hidden.astype(BF))

    def far_wave(w):
        sibling_arrived(w, far, NY - 1)
        multiply(w, far, False)
        down(w, (jax.nn.silu(acc[w, 0]) * acc[w, 1]).astype(BF))

    def gather_hop(hop, w):
        rights, lefts = turn(hop)
        arrived_gather(w, 0, hop - 1)
        if hop < H:
            gather_copy(w, 0, hop).start()
        arrived_gather(w, 1, hop - 1)
        if hop < H:
            gather_copy(w, 1, hop).start()
            sibling_copy(w, rights, 2 * hop - 1).start()
            sibling_copy(w, lefts, 2 * hop).start()
        else:
            sibling_copy(w, far, NY - 1).start()

    def at(s):
        return pl.ds(pl.multiple_of(s * 8, 8), 8)

    def summing(s, held):
        hf, pf, hb, pb = held
        a, b = af[at(s), :], bf[at(s), :]
        a2, b2 = ab[at(NS - 1 - s), :], bb[at(NS - 1 - s), :]
        return a * hf + b, a * pf, a2 * hb + b2, a2 * pb

    zero, one = jnp.zeros((8, LANES), F32), jnp.ones((8, LANES), F32)
    hf, pf, hb, pb = lax.fori_loop(0, NS, summing, (zero, one, zero, one), unroll=8)
    for k, value in enumerate((pf, hf, pb, hb)):
        seg[k] = value

    def segment(k, g):
        return seg[k, g : g + 1, :]

    ones = jnp.ones((1, LANES), F32)
    fa, fb, ba, bb_ = ones, ones * 0.0, ones, ones * 0.0
    for g in range(8):
        fa, fb = segment(0, g) * fa, segment(0, g) * fb + segment(1, g)
        ba, bb_ = segment(2, 7 - g) * ba, segment(2, 7 - g) * bb_ + segment(3, 7 - g)
    ahead = jnp.concatenate([fa, fb], axis=0)
    behind = jnp.concatenate([ba, bb_], axis=0)
    carry_send[0] = ahead
    carry_send[1] = behind
    carry_recv[e] = ahead

    def send_carry(i, _):
        peer = (e + i) % E
        pltpu.make_async_remote_copy(
            carry_send.at[(peer < e).astype(I32)], carry_recv.at[e], carry_ss, carry_rs,
            device_id=(peer, t), device_id_type=MESH,
        ).start()
        return 0

    lax.fori_loop(1, E, send_carry, 0)

    def second_pass():
        pltpu.make_async_copy(
            carry_recv.at[pl.ds(0, E - 1)], carry_recv.at[pl.ds(0, E - 1)], carry_rs
        ).wait()

        def fold(i, held):
            f, b = held
            one_way = carry_recv[i]
            j = E - 1 - i
            other = carry_recv[j]
            f = jnp.where(i < e, one_way[0:1] * f + one_way[1:2], f)
            b = jnp.where(j > e, other[0:1] * b + other[1:2], b)
            return f, b

        f, b = lax.fori_loop(0, E, fold, (ones * 0.0, ones * 0.0))
        f_rows, b_rows = [f], [b]
        for g in range(7):
            f_rows.append(segment(0, g) * f_rows[-1] + segment(1, g))
            b_rows.insert(0, segment(2, 7 - g) * b_rows[0] + segment(3, 7 - g))
        f_in, b_in = jnp.concatenate(f_rows, axis=0), jnp.concatenate(b_rows, axis=0)

        def states(s, held):
            hf, hb = held
            r = NS - 1 - s
            hf = af[at(s), :] * hf + bf[at(s), :]
            hb = ab[at(r), :] * hb + bb[at(r), :]
            bf[at(s), :] = hf
            bb[at(r), :] = hb
            return hf, hb

        lax.fori_loop(0, NS, states, (f_in, b_in), unroll=8)

        def natural(s, _):
            ynat[pl.ds(s, 8, stride=NS), :] = bf[at(s), :] + bb[at(s), :]
            return 0

        lax.fori_loop(0, NS, natural, 0, unroll=8)
        loads[13].wait()

        def finish(i, _):
            rows = pl.ds(pl.multiple_of(i * CH, CH), CH)
            rec_out[rows, :] = (ynat[rows, :] * jax.nn.gelu(gatev[rows, :].astype(F32))).astype(BF)
            return 0

        lax.fori_loop(0, S // CH, finish, 0)
        stores[0].start()

    near_arrived(0, 0, G)
    for load in loads[10:13]:
        load.wait()
    for hop in range(1, H):
        for w in range(2):
            gather_hop(hop, w)
        if hop == H - 2:
            near_arrived(1, 0, G // 2)
        if hop == H - 1:
            near_arrived(1, G // 2 if H > 2 else 0, G)
        if hop > 1:
            reduce_step(2, hop - 2)
        for w in range(2):
            multiply_hop(hop - 1, w)
        if hop == 1:
            near_wave(0)
    near_wave(1)
    for w in range(2):
        gather_hop(H, w)
        multiply_hop(H - 1, w)
    reduce_step(2, H - 2)
    reduce_step(3, 0)
    far_wave(0)
    far_wave(1)
    reduce_step(0, 0)
    reduce_step(2, H - 1)
    reduce_step(1, 0)
    reduce_step(3, 1)
    for step in range(1, H):
        reduce_step(0, step)
        reduce_step(1, step)
        if step == 1:
            send_back(2)
        if step + 1 < H:
            reduce_step(3, step + 1)
    send_back(3)
    send_back(0)
    send_back(1)
    loads[9].wait()
    shares_t = scores_t[...] / (scores_t[0:1, :] + scores_t[1:2, :])
    share_of = jnp.where(first_t, shares_t[0:1, :], 0.0) + jnp.where(second_t, shares_t[1:2, :], 0.0)
    own_row = t * EXIT + (iota((T * EXIT, R), 0) & (EXIT - 1))
    rows_out = one_hot(own_row == iota((T * EXIT, R), 1))
    columns_out = one_hot(iota((E, N), 0) == shr(iota((E, N), 1), lT))
    same_tile = shr(iota((T * EXIT, N), 0), 4) == (iota((T * EXIT, N), 1) & (T - 1))
    for w in range(2):
        weight = jnp.where(rank_t == float(w), share_of, 0.0)
        high = weight.astype(BF)
        low = (weight - high.astype(F32)).astype(BF)
        for piece, table in ((high, c_hi), (low, c_lo)):
            picked = lax.dot_general(rows_out, piece, (((1,), (1,)), ((), ())), preferred_element_type=F32)
            wide = dot(picked.astype(BF), columns_out)
            table[w] = jnp.where(same_tile, wide, 0.0).astype(BF)

    second_pass()
    tail.wait_send()
    head.wait_send()
    sent = [(carry_recv.at[pl.ds(0, E - 1)], carry_ss), (near_send.at[1], near_ss.at[1])]
    sent += [(dsp.at[w], dsp_ss.at[w]) for w in range(2)]
    sent += [(back.at[v], ret_ss.at[v]) for v in (0, 1, 3)]
    if G > 1:
        sent += [(near_send.at[0, pl.ds(0, GT - T)], near_ss.at[0])]
        sent += [(back.at[2, pl.ds(0, M - 2 * T)], ret_ss.at[2])]
    sent += [(xn.at[g, c], mate_ss.at[g]) for g in range(2)]
    for block, sem in sent:
        pltpu.make_async_copy(block, block, sem).wait()
    for w in range(2):
        for hop in range(H):
            for direction in range(2):
                gather_copy(w, direction, hop).wait_send()
        for index in range(NY):
            sibling_copy(w, y, index).wait_send()
    for v in range(4):
        for half in range(2):
            pair_copy(v, half).wait_send()
            for direction in range(2):
                for step in range(H):
                    if travels(direction, step, half):
                        sum_copy(v, direction, step, half).wait_send()
    arrivals = pl.ds(0, (E - 1) * T)
    out = jnp.zeros((T * EXIT, LANES), F32)
    for w in range(2):
        block = ret_recv.at[w, arrivals]
        pltpu.make_async_copy(block, block, ret_rs.at[w]).wait()
        out = out + dot(c_hi[w], ret_recv[w]) + dot(c_lo[w], ret_recv[w])
    for j in range(T):
        exp_out[:, j * LANES : (j + 1) * LANES] = out[j * EXIT : (j + 1) * EXIT, :].astype(BF)
    stores[1].start()

    for store in stores:
        store.wait()


def hand_over(rec_in, exp_in, rec_out, exp_out, rec, exp, in_sem, out_sem):
    loads = [
        pltpu.make_async_copy(rec_in, rec, in_sem.at[0]),
        pltpu.make_async_copy(exp_in, exp, in_sem.at[1]),
    ]
    stores = [
        pltpu.make_async_copy(rec, rec_out, out_sem.at[0]),
        pltpu.make_async_copy(exp, exp_out, out_sem.at[1]),
    ]
    for load in loads:
        load.start()
    for load, store in zip(loads, stores):
        load.wait()
        store.start()
    for store in stores:
        store.wait()


def local(
    E, T, x_path, gate_path, conv_taps, decay_gate_w, input_gate_w, decay_rate, decay_shift,
    expert_in, norm_gain, routes, route_scores, gate_weight, up_weight, down_weight,
):
    S = x_path.shape[0]
    R, D = expert_in.shape
    F = gate_weight.shape[2]
    NY, H, K, G, HALF = T // 2, T // 4, E // 2, E // 4, D // 2
    N, M = E * T, K * T
    hbm = pl.BlockSpec(memory_space=pltpu.HBM)
    dma = pltpu.SemaphoreType.DMA
    rows = pltpu.VMEM((S, LANES), F32)
    scratch = [
        pltpu.VMEM((S, LANES), BF),
        pltpu.VMEM((S, LANES), BF),
        pltpu.VMEM((R, D), BF),
        pltpu.VMEM((D, F), BF),
        pltpu.VMEM((D, F), BF),
        pltpu.VMEM((F, D), BF),
        pltpu.VMEM((4, LANES), F32),
        pltpu.VMEM((2, 1, LANES, LANES), BF),
        pltpu.VMEM((2, 1, LANES, LANES), BF),
        pltpu.VMEM((2, LANES), F32),
        pltpu.VMEM((8, S // 8), F32),
        pltpu.VMEM((D // LANES, LANES), F32),
        pltpu.VMEM((2, R), I32),
        pltpu.VMEM((2, R), F32),
        pltpu.VMEM((S, LANES), BF),
        pltpu.VMEM((EXIT, D), BF),
        pltpu.VMEM((2, EXIT, LANES), BF),
        pltpu.VMEM((S + 2 * EXIT, LANES), F32),
        rows,
        rows,
        rows,
        rows,
        rows,
        rows,
        rows,
        pltpu.VMEM((4, 8, LANES), F32),
        pltpu.VMEM((2, 2, LANES), F32),
        pltpu.VMEM((E, 2, LANES), F32),
        pltpu.VMEM((2, E, R), F32),
        pltpu.VMEM((2, M, R), BF),
        pltpu.VMEM((M, R), BF),
        pltpu.VMEM((R, D), BF),
        pltpu.VMEM((2, M, LANES), BF),
        pltpu.VMEM((2, M // 2, D), BF),
        pltpu.VMEM((2, NY, 2, M, LANES), BF),
        pltpu.VMEM((2, 2, M // 2, D), BF),
        pltpu.VMEM((2, 2, M, F), F32),
        pltpu.VMEM((M, M), BF),
        pltpu.VMEM((M, F), BF),
        pltpu.VMEM((4, 2, 2, NY, K, HALF), BF),
        pltpu.VMEM((4, 2, NY, K, HALF), BF),
        pltpu.VMEM((4, 2, H, 2, K, HALF), BF),
        pltpu.VMEM((4, 2, H, 2, K, HALF), BF),
        pltpu.VMEM((M, LANES), F32),
        pltpu.VMEM((4, M, LANES), BF),
        pltpu.VMEM((2, N, LANES), BF),
        pltpu.VMEM((2, T * EXIT, N), BF),
        pltpu.VMEM((2, T * EXIT, N), BF),
        dma((14,)),
        dma((2,)),
        dma((2,)),
        dma((2,)),
        dma,
        dma,
        dma((2,)),
        dma((2,)),
        dma((2,)),
        dma((2, G)),
        dma((2,)),
        dma((2,)),
        dma((2, 2, H)),
        dma((2, 2, H)),
        dma((2, NY)),
        dma((2, NY)),
        dma((4, 2)),
        dma((4, 2)),
        dma((4, 2, H, 2)),
        dma((4, 2, H, 2)),
        dma((4,)),
        dma((2,)),
    ]
    results = pl.pallas_call(
        functools.partial(layer, E, T),
        out_shape=(
            jax.ShapeDtypeStruct((S, LANES), BF),
            jax.ShapeDtypeStruct((EXIT, D), BF),
        ),
        in_specs=[hbm] * 14,
        out_specs=(hbm, hbm),
        scratch_shapes=scratch,
        compiler_params=pltpu.CompilerParams(
            collective_id=0, has_side_effects=True, vmem_limit_bytes=60 * 1024 * 1024
        ),
        name="layer",
    )(
        x_path,
        gate_path,
        expert_in,
        gate_weight.reshape(D, F),
        up_weight.reshape(D, F),
        down_weight.reshape(F, D),
        conv_taps,
        decay_gate_w,
        input_gate_w,
        decay_rate,
        decay_shift.reshape(8, S // 8),
        norm_gain.reshape(D // LANES, LANES),
        routes.T,
        route_scores.T,
    )
    return pl.pallas_call(
        hand_over,
        out_shape=tuple(jax.ShapeDtypeStruct(r.shape, r.dtype) for r in results),
        in_specs=[hbm] * 2,
        out_specs=(hbm, hbm),
        scratch_shapes=[pltpu.VMEM(r.shape, r.dtype) for r in results] + [dma((2,)), dma((2,))],
        compiler_params=pltpu.CompilerParams(vmem_limit_bytes=60 * 1024 * 1024),
        name="hand_over",
    )(*results)


def solution(mesh):
    in_specs = (
        P("ep", "tp"),
        P("ep", "tp"),
        P(None, "tp"),
        P(None, "tp", None, None),
        P(None, "tp", None, None),
        P(None, "tp"),
        P("ep", "tp"),
        P("ep", None),
        P(),
        P("ep", None),
        P("ep", None),
        P("ep", None, "tp"),
        P("ep", None, "tp"),
        P("ep", "tp", None),
    )
    out_specs = (P("ep", "tp"), P(("ep", "tp"), None))
    step = functools.partial(local, mesh.shape["ep"], mesh.shape["tp"])
    return jax.shard_map(step, mesh=mesh, in_specs=in_specs, out_specs=out_specs, check_vma=False)
```
